512 devices in a mesh: rep: 2 (over z_hi), fs: 32 (over z_lo, y), tp: 8 (over x, core).
Axes of the slice: x: 4, y: 8, z: 8 (z_hi: 2, z_lo: 4; z = z_hi * 4 + z_lo), core: 2. Of those that a mesh axis runs over, the one named last changes fastest.
Arguments:
- residual: bfloat16 [2048, 16384], P('tp', ('rep', 'fs')), may hold values from -6 to 6
- mixer_gain: float32 [2048], replicated, may hold values from 0.1 to 1.9
- value_weight: float32 [2048, 512], P('fs', 'tp'), may hold values from -0.125 to 0.125
- value_scale: float32 [512], P('tp'), may hold values from 0.2 to 8, as said below
- input_gate_weight: float32 [2048, 512], P('fs', 'tp'), may hold values from -0.125 to 0.125
- input_gate_scale: float32 [512], P('tp'), may hold values from 0.5 to 2
- output_gate_weight: float32 [2048, 512], P('fs', 'tp'), may hold values from -0.125 to 0.125
- output_gate_scale: float32 [512], P('tp'), may hold values from 0.5 to 2
- conv_taps: float32 [3, 512], P(None, 'tp'), may hold values from -3 to 3
- conv_gain: float32 [512], P('tp'), may hold values from 0.1 to 1.9
- mixer_out_weight: float32 [512, 2048], P('tp', 'fs'), may hold values from -0.25 to 0.25
- mixer_out_scale: float32 [2048], P('fs'), may hold values from 0.5 to 2
- channel_gain: float32 [2048], replicated, may hold values from 0.1 to 1.9
- gate_weight: float32 [2048, 5632], P('fs', 'tp'), may hold values from -0.125 to 0.125
- gate_scale: float32 [5632], P('tp'), may hold values from 0.5 to 2
- up_weight: float32 [2048, 5632], P('fs', 'tp'), may hold values from -0.125 to 0.125
- up_scale: float32 [5632], P('tp'), may hold values from 0.5 to 2
- down_weight: float32 [5632, 2048], P('tp', 'fs'), may hold values from -0.078125 to 0.078125
- down_scale: float32 [2048], P('fs'), may hold values from 0.5 to 2
Outputs:
- layer_out: bfloat16 [2048, 16384], P('tp', ('rep', 'fs'))
The draws below stay inside these ranges and needn't reach their ends.
Inputs may be any that keep to these rules, and one draw needn't show every extreme that they name: `value_scale`: positive column scales.
All inputs are finite; a program needn't handle non-finite values.
Results may differ from the reference program's by a relative error of at most 0.018.
Values may be sent and summed in bfloat16 or wider, within the bound.
A program may use at most 64 MiB of HBM per device.

```python
import math
import jax
import jax.numpy as jnp
from jax import lax

D = 2048
C = 512
FF = 5632
TAPS = 3
LEN = 128
TOKENS = 16384
N_TP = 8


def draw_value_scale(key, part):
    index = jnp.arange(C, dtype=jnp.float32)
    ramp = 4.0 ** (index / C)
    rough = jnp.exp(jax.random.uniform(key, (C,), jnp.float32, -0.7, 0.7))
    return (0.5 * ramp * rough).astype(jnp.float32)


def shard_levels(own_key, shape, split, smallest, top_value):
    loudness = 1.0
    for dim, shards_of in split:
        heights = jax.random.uniform(jax.random.fold_in(jax.random.fold_in(own_key, 6), dim), (shards_of,), jnp.float32, smallest / len(split), top_value / len(split))
        loudness = loudness * jnp.repeat(jnp.exp(heights), shape[dim] // shards_of).reshape((-1,) + (1,) * (len(shape) - 1 - dim))
    return loudness


def scatter_about(own_key, extent, scale, most, pieces=(), kind=jnp.bfloat16):
    factor_of = shard_levels(own_key, extent, pieces, -0.22, 0.18) if pieces else 1.0
    values = jax.random.normal(own_key, extent, jnp.float32) * scale * factor_of
    return jnp.minimum(jnp.maximum(values, -most), most).astype(kind)


def setup_inputs(seed: int = 0) -> dict:
    key_of = jax.random.split(jax.random.key(seed), 20)
    residual = scatter_about(key_of[0], (D, TOKENS), 1.0, 6.0, ((0, 8), (1, 64)))
    mixer_gain = jnp.clip(1.0 + 0.18 * jax.random.normal(key_of[1], (D,), jnp.float32), 0.1, 1.9)
    value_weight = scatter_about(key_of[2], (D, C), D ** -0.5, 0.125, ((0, 32), (1, 8)), jnp.float32)
    value_scale = draw_value_scale(jax.random.fold_in(key_of[19], 71), 0)
    input_gate_weight = scatter_about(key_of[4], (D, C), D ** -0.5, 0.125, ((0, 32), (1, 8)), jnp.float32)
    input_gate_scale = jnp.clip(jnp.exp(math.log(2.0) - 1.3862944 * jax.random.uniform(key_of[5], (C,), jnp.float32) ** shard_levels(key_of[5], (C,), ((0, 8),), -0.2, 0.2)), 0.5, 2.0)
    output_gate_weight = scatter_about(key_of[6], (D, C), D ** -0.5, 0.125, ((0, 32), (1, 8)), jnp.float32)
    output_gate_scale = jnp.clip(jnp.exp(math.log(2.0) - 1.3862944 * jax.random.uniform(key_of[7], (C,), jnp.float32) ** shard_levels(key_of[7], (C,), ((0, 8),), -0.2, 0.2)), 0.5, 2.0)
    conv_taps = scatter_about(key_of[8], (TAPS, C), 0.577, 3.0, ((1, 8),), jnp.float32)
    conv_gain = jnp.clip(1.0 + 0.18 * jax.random.normal(key_of[9], (C,), jnp.float32), 0.1, 1.9)
    mixer_out_weight = scatter_about(key_of[10], (C, D), C ** -0.5, 0.25, ((0, 8), (1, 32)), jnp.float32)
    mixer_out_scale = jnp.clip(jnp.exp(math.log(2.0) - 1.3862944 * jax.random.uniform(key_of[11], (D,), jnp.float32) ** shard_levels(key_of[11], (D,), ((0, 32),), -0.2, 0.2)), 0.5, 2.0)
    channel_gain = jnp.clip(1.0 + 0.18 * jax.random.normal(key_of[12], (D,), jnp.float32), 0.1, 1.9)
    gate_weight = scatter_about(key_of[13], (D, FF), D ** -0.5, 0.125, ((0, 32), (1, 8)), jnp.float32)
    gate_scale = jnp.clip(jnp.exp(math.log(2.0) - 1.3862944 * jax.random.uniform(key_of[14], (FF,), jnp.float32) ** shard_levels(key_of[14], (FF,), ((0, 8),), -0.2, 0.2)), 0.5, 2.0)
    up_weight = scatter_about(key_of[15], (D, FF), D ** -0.5, 0.125, ((0, 32), (1, 8)), jnp.float32)
    up_scale = jnp.clip(jnp.exp(math.log(2.0) - 1.3862944 * jax.random.uniform(key_of[16], (FF,), jnp.float32) ** shard_levels(key_of[16], (FF,), ((0, 8),), -0.2, 0.2)), 0.5, 2.0)
    down_weight = scatter_about(key_of[17], (FF, D), FF ** -0.5, 0.078125, ((0, 8), (1, 32)), jnp.float32)
    down_scale = jnp.clip(jnp.exp(math.log(2.0) - 1.3862944 * jax.random.uniform(key_of[18], (D,), jnp.float32) ** shard_levels(key_of[18], (D,), ((0, 32),), -0.2, 0.2)), 0.5, 2.0)
    return dict(residual=residual, mixer_gain=mixer_gain, value_weight=value_weight, value_scale=value_scale, input_gate_weight=input_gate_weight, input_gate_scale=input_gate_scale, output_gate_weight=output_gate_weight, output_gate_scale=output_gate_scale, conv_taps=conv_taps, conv_gain=conv_gain, mixer_out_weight=mixer_out_weight, mixer_out_scale=mixer_out_scale, channel_gain=channel_gain, gate_weight=gate_weight, gate_scale=gate_scale, up_weight=up_weight, up_scale=up_scale, down_weight=down_weight, down_scale=down_scale)


epsilon = 1e-06

def normalize(values, gain):
    floats = values.astype(jnp.float32)
    mean = lax.optimization_barrier(jnp.mean(floats * floats, axis=0, keepdims=True))
    return (floats * lax.rsqrt(mean + epsilon) * gain[:, None]).astype(jnp.bfloat16)

def project(weight, rows):
    return jnp.dot(weight.T, rows, preferred_element_type=jnp.float32)

def causal_conv(values, taps):
    total = values.shape[1]
    position = jnp.arange(total, dtype=jnp.int32) % LEN
    shifted_one = jnp.pad(values, ((0, 0), (1, 0)))[:, :total]
    shifted_two = jnp.pad(values, ((0, 0), (2, 0)))[:, :total]
    shifted_one = jnp.where(position[None, :] >= 1, shifted_one, 0.0)
    shifted_two = jnp.where(position[None, :] >= 2, shifted_two, 0.0)
    return taps[2][:, None] * values + taps[1][:, None] * shifted_one + taps[0][:, None] * shifted_two

def block_sum(weight, rows, scale):
    width = weight.shape[0] // N_TP
    total = jnp.zeros((weight.shape[1], rows.shape[1]), jnp.float32)
    for block_index in range(N_TP):
        lower = block_index * width
        part = project(weight[lower:lower + width], rows[lower:lower + width]) * scale[:, None]
        rounded = lax.optimization_barrier(part.astype(jnp.bfloat16))
        total = total + rounded.astype(jnp.float32)
    return total

def reference(residual, mixer_gain, value_weight, value_scale, input_gate_weight, input_gate_scale, output_gate_weight, output_gate_scale, conv_taps, conv_gain, mixer_out_weight, mixer_out_scale, channel_gain, gate_weight, gate_scale, up_weight, up_scale, down_weight, down_scale):
    normed = normalize(residual, mixer_gain)
    value = project(value_weight.astype(jnp.bfloat16), normed) * value_scale[:, None]
    in_gate = project(input_gate_weight.astype(jnp.bfloat16), normed) * input_gate_scale[:, None]
    out_gate = project(output_gate_weight.astype(jnp.bfloat16), normed) * output_gate_scale[:, None]
    mixed = out_gate * causal_conv(in_gate * value, conv_taps)
    mean = lax.optimization_barrier(jnp.mean(mixed * mixed, axis=0, keepdims=True))
    conv_normed = (mixed * lax.rsqrt(mean + epsilon) * conv_gain[:, None]).astype(jnp.bfloat16)
    total = block_sum(mixer_out_weight.astype(jnp.bfloat16), conv_normed, mixer_out_scale)
    after_mixer = (residual.astype(jnp.float32) + total).astype(jnp.bfloat16)
    normed_two = normalize(after_mixer, channel_gain)
    gate = project(gate_weight.astype(jnp.bfloat16), normed_two) * gate_scale[:, None]
    upper = project(up_weight.astype(jnp.bfloat16), normed_two) * up_scale[:, None]
    hidden = (jax.nn.silu(gate) * upper).astype(jnp.bfloat16)
    total_two = block_sum(down_weight.astype(jnp.bfloat16), hidden, down_scale)
    return (after_mixer.astype(jnp.float32) + total_two).astype(jnp.bfloat16)
```

```python
import functools

import jax
import jax.numpy as jnp
from jax import lax
from jax.experimental import pallas as pl
from jax.experimental.pallas import tpu as pltpu
from jax.sharding import PartitionSpec as P

MESH = pl.DeviceIdType.MESH
F32 = jnp.float32
BF = jnp.bfloat16
EPS = 1e-06
LEN = 128
T = 256
NM, NG, ND = 256, 1408, 768
FFL = 704
ST = 272


class Event:
    def __init__(self, name, link, size, deps, put, got):
        self.name, self.link, self.size, self.deps = name, link, size, deps
        self.put, self.got = put, got


RATE = {"p": 300.0, "xx": 23.0}
LAT = {"p": 1.0, "xx": 2.6}


def plan(events, tasks):
    done, order, sent, flights = set(), [], set(), []
    free = {}
    now = 0.0

    def launch():
        for e in events:
            if e.name not in sent and all(d in done for d in e.deps):
                sent.add(e.name)
                start = max(now, free.get(e.link, 0.0))
                end = start + e.size / (RATE.get(e.link, 46.0) * 1e3)
                free[e.link] = end
                flights.append((end + LAT.get(e.link, 1.8), e))
                order.append(("send", e))

    launch()
    left = list(tasks)
    while flights or left:
        ready = [t for t in left if all(d in done for d in t[1])]
        landed = [f for f in flights if f[0] <= now]
        if landed:
            f = min(landed, key=lambda v: v[0])
        elif ready:
            t = ready[0]
            left.remove(t)
            order.append(("run", t))
            now += t[2]
            done.add(t[0])
            launch()
            continue
        else:
            f = min(flights, key=lambda v: v[0])
            now = f[0]
        flights.remove(f)
        order.append(("wait", f[1]))
        done.add(f[1].name)
        launch()
    return order


def weight_events(M, D, G, W):
    ev = []

    def add(name, link, size, deps, ref):
        ev.append(Event(name, link, size, deps, lambda: ref(*W.shift[link]), lambda: ref(0, 0)))

    def along_z(tag, buf, width, b, have, first):
        size = 64 * width * 2
        for sign, link in ((-1, "z+"), (1, "z-")):
            add(f"{tag}{link}1", link, size, have, lambda dz, dy, s=sign: buf.at[W.zl(s + dz), W.yy(b + dy)])
        for sign, link, lo in ((-1, "z+", 0), (1, "z-", 32)):
            add(f"{tag}{link}2", link, size // 2, [f"{tag}{link}1"],
                lambda dz, dy, s=sign, lo=lo: buf.at[W.zl(2 * s + dz), W.yy(b + dy), pl.ds(lo, 32)])
        return [f"{tag}z+1", f"{tag}z-1", f"{tag}z+2", f"{tag}z-2"]

    mz = along_z("M", M, NM, 0, ["initM"], True)
    all_m = list(mz)
    for s in (1, 2, 3, 4):
        for sign, link, lo in ((-1, "y+", 0), (1, "y-", 2)):
            deps = mz + ["initM"] if s == 1 else [f"My{link}{s - 1}"]
            n = 4 if s < 4 else 2
            at = 0 if s < 4 else lo
            add(f"My{link}{s}", link, n * 64 * NM * 2, deps,
                lambda dz, dy, s=s, sign=sign, at=at, n=n: M.at[pl.ds(at, n), W.yy(sign * s + dy)])
            all_m.append(f"My{link}{s}")
    all_g = []
    for s in (1, 2, 3, 4):
        for sign, link, lo in ((-1, "y+", 0), (1, "y-", 32)):
            deps = ["initG"] if s == 1 else [f"Gy{link}{s - 1}"]
            n = 64 if s < 4 else 32
            at = 0 if s < 4 else lo
            add(f"Gy{link}{s}", link, n * NG * 2, deps,
                lambda dz, dy, s=s, sign=sign, at=at, n=n: G.at[W.zl(dz), W.yy(sign * s + dy), pl.ds(at, n)])
            all_g.append(f"Gy{link}{s}")
    for b in (0, -1, 1, -2, 2, -3, 3, 4):
        if b == 0:
            have = ["initG"]
        elif b == 4:
            have = ["Gyy+4", "Gyy-4"]
        else:
            have = [f"Gyy+{-b}"] if b < 0 else [f"Gyy-{b}"]
        all_g += along_z(f"G{b}", G, NG, b, have, False)
    all_d = along_z("D", D, ND, 0, ["initD"], True)
    dz_names = list(all_d)
    for s in (1, 2, 3, 4):
        for g in (0, 1):
            for sign, link in ((-1, "y+"), (1, "y-")):
                if s == 4 and (g == 0) != (link == "y+"):
                    continue
                deps = dz_names + ["initD"] if s == 1 else [f"Dy{link}{s - 1}g{g}"]
                add(f"Dy{link}{s}g{g}", link, 2 * 64 * ND * 2, deps,
                    lambda dz, dy, s=s, sign=sign, g=g: D.at[pl.ds(2 * g, 2), W.yy(sign * s + dy)])
                all_d.append(f"Dy{link}{s}g{g}")
    return ev, all_m, all_g, all_d


class Where:
    pass


def kernel(m_in, g_in, d_in, xt_in, res, small, gus, gains, out,
           M, G, D, X1, X2, XN, acc, hid, keep, own32, preo, prei, rxo, rxi, qo, qi, ro, ri,
           send_sem, recv_sem, loc_sem, n_events):
    rep, fs, tp = lax.axis_index("rep"), lax.axis_index("fs"), lax.axis_index("tp")
    y, zl = lax.rem(fs, 8), lax.div(fs, 8)
    x, c = lax.div(tp, 2), lax.rem(tp, 2)
    z = rep * 4 + zl

    def y_at(d):
        return {"fs": zl * 8 + lax.rem(y + d + 8, 8)}

    def z_at(d):
        zz = lax.rem(z + d + 8, 8)
        return {"rep": lax.div(zz, 4), "fs": lax.rem(zz, 4) * 8 + y}

    def x_at(d):
        return {"tp": lax.rem(x + d + 4, 4) * 2 + c}

    partner = {"tp": x * 2 + 1 - c}
    target = {"y+": y_at(1), "y-": y_at(-1), "z+": z_at(1), "z-": z_at(-1),
              "x+": x_at(1), "x-": x_at(-1), "xx": x_at(2), "p": partner}

    W = Where()
    W.shift = {"y+": (0, 1), "y-": (0, -1), "z+": (1, 0), "z-": (-1, 0)}
    W.shift = {"y+": (0, 1), "y-": (0, -1), "z+": (1, 0), "z-": (-1, 0)}
    W.zl = lambda d: lax.rem(zl + d + 8, 4)
    W.yy = lambda d: lax.rem(y + d + 16, 8)

    ev, all_m, all_g, all_d = weight_events(M, D, G, W)
    pos = {"x+": -1, "x-": 1, "xx": 2}

    def slot(d, core):
        return lax.rem(x + d + 4, 4) * 2 + core

    def spread(tag, buf, first):
        names = []
        for link in ("x+", "x-", "xx"):
            ev.append(Event(f"{tag}{link}", link, T * 256 * 2, [first],
                            lambda: buf.at[slot(0, c)], lambda link=link: buf.at[slot(pos[link], c)]))
            names.append(f"{tag}{link}")
        ev.append(Event(f"{tag}p", "p", T * 256 * 2, [first],
                        lambda: buf.at[slot(0, c)], lambda: buf.at[slot(0, 1 - c)]))
        names.append(f"{tag}p")
        for link in ("x+", "x-", "xx"):
            ev.append(Event(f"{tag}p{link}", "p", T * 256 * 2, [f"{tag}{link}"],
                            lambda link=link: buf.at[slot(pos[link], c)],
                            lambda link=link: buf.at[slot(pos[link], 1 - c)]))
            names.append(f"{tag}p{link}")
        return names

    all_x1 = spread("X1", X1, "initX")
    hop = {"x+": 1, "x-": 3, "xx": 2}
    ev.append(Event("Q", "p", 4 * ST * T * 2, ["mix"], lambda: preo, lambda: prei))
    for link, j in hop.items():
        ev.append(Event(f"R{link}", link, ST * T * 2, ["mixsum"],
                        lambda j=j: rxo.at[j - 1], lambda j=j: rxi.at[j - 1]))
    all_x2 = spread("X2", X2, "after")
    for j in range(4):
        ev.append(Event(f"S{j}", "p", 256 * T * 2, [f"down{j}"], lambda j=j: qo.at[j], lambda j=j: qi.at[j]))
    for link, j in hop.items():
        ev.append(Event(f"U{link}", link, 256 * T * 2, [f"sum{j}"],
                        lambda j=j: ro.at[j - 1], lambda j=j: ri.at[j - 1]))
    assert len(ev) == n_events, len(ev)
    index = {e.name: i for i, e in enumerate(ev)}

    barrier = pltpu.get_barrier_semaphore()
    for dev in target.values():
        pl.semaphore_signal(barrier, inc=1, device_id=dev, device_id_type=MESH)

    def local_copy(i, src, dst):
        return pltpu.make_async_copy(src, dst, loc_sem.at[i])

    inits = [local_copy(0, m_in, M.at[zl, y]), local_copy(1, g_in, G.at[zl, y]),
             local_copy(2, d_in, D.at[zl, y]), local_copy(3, xt_in, X1.at[slot(0, c)])]
    for i in inits:
        i.start()
    for i in inits:
        i.wait()
    pl.semaphore_wait(barrier, 8)

    def start(e):
        i = index[e.name]
        ref = e.put()
        pltpu.make_async_remote_copy(src_ref=ref, dst_ref=ref if e.link[0] in "yz" or e.name[:1] == "X" else e.got(),
                                     send_sem=send_sem.at[i], recv_sem=recv_sem.at[i],
                                     device_id=target[e.link], device_id_type=MESH).start()

    def arrive(e):
        i = index[e.name]
        ref = e.got()
        pltpu.make_async_remote_copy(src_ref=ref, dst_ref=ref, send_sem=send_sem.at[i], recv_sem=recv_sem.at[i],
                                     device_id=target[e.link], device_id_type=MESH).wait_recv()

    def left(e):
        i = index[e.name]
        ref = e.put()
        pltpu.make_async_remote_copy(src_ref=ref, dst_ref=ref, send_sem=send_sem.at[i], recv_sem=recv_sem.at[i],
                                     device_id=target[e.link], device_id_type=MESH).wait_send()

    def normed(buf, row):
        def square(k, s):
            v = buf[k].astype(F32)
            return s + v * v
        total = lax.fori_loop(0, 8, square, jnp.zeros((T, 256), F32))
        factor = lax.rsqrt(jnp.sum(total, axis=1, keepdims=True) * (1.0 / 2048) + EPS)
        for k in range(8):
            cols = slice(k * 256, k * 256 + 256)
            XN[:, cols] = (buf[k].astype(F32) * factor * gains[row:row + 1, cols]).astype(BF)

    def norm_one():
        normed(X1, 0)

    def split_stats(s):
        high = s.astype(BF)
        low = (s - high.astype(F32)).astype(BF)
        return jnp.concatenate([high, low], axis=0)

    def mix():
        proj = jnp.dot(XN[...], M[...].reshape(2048, NM), preferred_element_type=F32)
        first, second = proj[:, :128], proj[:, 128:]
        u = first * pltpu.roll(first, 64, axis=1)
        place = lax.rem(lax.broadcasted_iota(jnp.int32, (T, 128), 0), LEN)
        lane = lax.broadcasted_iota(jnp.int32, (T, 128), 1)
        one = jnp.where(place >= 1, pltpu.roll(u, 1, axis=0), 0.0)
        two = jnp.where(place >= 2, pltpu.roll(u, 2, axis=0), 0.0)
        conv = small[2:3] * u + small[1:2] * one + small[0:1] * two
        mixed = jnp.where(lane >= 64, pltpu.roll(second, 64, axis=1) * conv, 0.0)
        sq = mixed * mixed
        high = sq.astype(BF)
        low = (sq - high.astype(F32)).astype(BF)
        ones = jnp.ones((16, 128), BF)
        nt = (((1,), (1,)), ((), ()))
        stat = (lax.dot_general(ones, high, nt, preferred_element_type=F32)
                + lax.dot_general(ones, low, nt, preferred_element_type=F32))[:8]
        scaled = (mixed * small[3:4]).astype(BF)
        for j in range(4):
            for mine in (False, True):
                core = c if mine else 1 - c
                w = M[lax.rem(x + j, 4), pl.ds(4 * core, 4), :, 128:].reshape(256, 128)
                part = lax.dot_general(w, scaled, nt, preferred_element_type=F32)
                if mine:
                    own32[j] = part
                else:
                    preo[j, :256] = part.astype(BF)
                    preo[j, 256:] = split_stats(stat)
        keep[0:8] = stat

    def mixsum():
        stat = keep[0:8] + prei[0, 256:264].astype(F32) + prei[0, 264:272].astype(F32)
        for j in (2, 1, 3):
            rxo[j - 1, :256] = (own32[j] + prei[j, :256].astype(F32)).astype(BF)
            rxo[j - 1, 256:] = split_stats(stat)
        own32[0] = own32[0] + prei[0, :256].astype(F32)
        keep[0:8] = stat

    def after():
        stat = keep[0:8]
        total = own32[0]
        for j in range(3):
            total = total + rxi[j, :256].astype(F32)
            stat = stat + rxi[j, 256:264].astype(F32) + rxi[j, 264:272].astype(F32)
        factor = lax.rsqrt(stat * (1.0 / 512) + EPS)[0:1]
        value = (res[...].astype(F32) + total * factor).astype(BF)
        X2[slot(0, c)] = value.astype(F32).T.astype(BF)
        out[...] = value

    def norm_two():
        normed(X2, 1)

    def hidden():
        for n in range(6):
            cols = slice(n * 256, min(n * 256 + 256, NG))
            w = G[:, :, :, cols].reshape(2048, cols.stop - cols.start)
            acc[:, cols] = jnp.dot(XN[...], w, preferred_element_type=F32) * gus[0:1, cols]
        lane = lax.broadcasted_iota(jnp.int32, (T, 128), 1)
        for n in range(6):
            even = acc[:, 256 * n:256 * n + 128]
            if n < 5:
                odd = acc[:, 256 * n + 128:256 * n + 256]
            else:
                odd = jnp.zeros((T, 128), F32)
            gate = jnp.where(lane < 64, even, odd)
            up = pltpu.roll(jnp.where(lane < 64, odd, even), 64, axis=1)
            hid[:, 128 * n:128 * n + 128] = (gate / (1.0 + jnp.exp(-gate)) * up).astype(BF)

    def down(j, core):
        w = D[lax.rem(x + j, 4), pl.ds(4 * core, 4)].reshape(256, ND)
        return lax.dot_general(w, hid[...], (((1,), (1,)), ((), ())), preferred_element_type=F32)

    def down_partner(j):
        qo[j] = down(j, 1 - c).astype(BF)

    def down_own():
        for j in range(4):
            own32[j] = down(j, c)

    def sum_for(j):
        ro[j - 1] = (own32[j] + qi[j].astype(F32)).astype(BF)

    def final():
        total = own32[0] + qi[0].astype(F32)
        for j in range(3):
            total = total + ri[j].astype(F32)
        out[...] = (out[...].astype(F32) + total).astype(BF)

    tasks = [
        ("norm1", all_x1, 2.0, norm_one),
        ("mix", ["norm1"] + all_m, 2.5, mix),
        ("mixsum", ["Q"], 0.7, mixsum),
        ("after", ["Rx+", "Rx-", "Rxx"], 0.7, after),
        ("norm2", all_x2, 2.0, norm_two),
        ("hidden", ["norm2"] + all_g, 4.0, hidden),
        ("down2", ["hidden"] + all_d, 0.3, lambda: down_partner(2)),
        ("down1", ["down2"], 0.3, lambda: down_partner(1)),
        ("down3", ["down1"], 0.3, lambda: down_partner(3)),
        ("down0", ["down3"], 0.3, lambda: down_partner(0)),
        ("own", ["down0"], 1.0, down_own),
        ("sum2", ["own", "S2"], 0.2, lambda: sum_for(2)),
        ("sum1", ["own", "S1"], 0.2, lambda: sum_for(1)),
        ("sum3", ["own", "S3"], 0.2, lambda: sum_for(3)),
        ("final", ["S0", "Ux+", "Ux-", "Uxx"], 0.5, final),
    ]
    order = plan_from(ev, tasks)
    for kind, item in order:
        if kind == "send":
            start(item)
        elif kind == "wait":
            arrive(item)
        else:
            item[3]()
    for e in ev:
        left(e)


def plan_from(events, tasks):
    for e in events:
        e.deps = [d for d in e.deps if not d.startswith("init")]
    return plan(events, tasks)


N_EVENTS = 12 + 40 + 18 + 7 + 1 + 3 + 7 + 4 + 3


def local(residual, mixer_gain, value_weight, value_scale, input_gate_weight, input_gate_scale,
          output_gate_weight, output_gate_scale, conv_taps, conv_gain, mixer_out_weight, mixer_out_scale,
          channel_gain, gate_weight, gate_scale, up_weight, up_scale, down_weight, down_scale):
    m = jnp.concatenate([value_weight, input_gate_weight, output_gate_weight,
                         mixer_out_weight.T * mixer_out_scale[:, None]], axis=1).astype(BF)
    even = (jnp.arange(11) % 2 == 0)[:, None]

    def laced(a, b):
        a = a.reshape(*a.shape[:-1], 11, 64)
        b = b.reshape(*b.shape[:-1], 11, 64)
        both = jnp.concatenate([jnp.where(even, a, b), jnp.where(even, b, a)], axis=-1)
        return both.reshape(*both.shape[:-2], NG)

    g = laced(gate_weight.astype(BF), up_weight.astype(BF))
    gus = jnp.broadcast_to(laced(gate_scale, up_scale)[None], (8, NG))
    d = jnp.pad((down_weight.T * down_scale[:, None]).astype(BF), ((0, 0), (0, ND - FFL)))
    factor = value_scale * input_gate_scale * output_gate_scale
    rows = jnp.concatenate([conv_taps * factor[None], conv_gain[None], jnp.zeros((4, 64), F32)], axis=0)
    small = jnp.concatenate([rows, rows], axis=1)
    gains = jnp.concatenate([mixer_gain[None], channel_gain[None], jnp.zeros((6, 2048), F32)], axis=0)
    hbm = pl.BlockSpec(memory_space=pl.ANY)
    vmem = pl.BlockSpec(memory_space=pltpu.VMEM)
    V = pltpu.VMEM
    return pl.pallas_call(
        functools.partial(kernel, n_events=N_EVENTS),
        out_shape=jax.ShapeDtypeStruct((256, T), BF),
        in_specs=[hbm] * 4 + [vmem] * 4,
        out_specs=vmem,
        scratch_shapes=[
            V((4, 8, 64, NM), BF), V((4, 8, 64, NG), BF), V((4, 8, 64, ND), BF),
            V((8, T, 256), BF), V((8, T, 256), BF), V((T, 2048), BF), V((T, NG), F32), V((T, ND), BF),
            V((8, T), F32), V((4, 256, T), F32),
            V((4, ST, T), BF), V((4, ST, T), BF), V((3, ST, T), BF), V((3, ST, T), BF),
            V((4, 256, T), BF), V((4, 256, T), BF), V((3, 256, T), BF), V((3, 256, T), BF),
            pltpu.SemaphoreType.DMA((N_EVENTS,)), pltpu.SemaphoreType.DMA((N_EVENTS,)),
            pltpu.SemaphoreType.DMA((4,)),
        ],
        compiler_params=pltpu.CompilerParams(collective_id=0, has_side_effects=True,
                                             vmem_limit_bytes=60 * 1024 * 1024),
        name="layer",
    )(m, g, d, residual.T, residual, small, gus, gains)


def solution(mesh):
    rf = ("rep", "fs")
    in_specs = (P("tp", rf), P(), P("fs", "tp"), P("tp"), P("fs", "tp"), P("tp"), P("fs", "tp"), P("tp"),
                P(None, "tp"), P("tp"), P("tp", "fs"), P("fs"), P(), P("fs", "tp"), P("tp"), P("fs", "tp"),
                P("tp"), P("tp", "fs"), P("fs"))
    return jax.shard_map(local, mesh=mesh, in_specs=in_specs, out_specs=P("tp", rf), check_vma=False)
```

```python
import functools

import jax
import jax.numpy as jnp
from jax import lax
from jax.experimental import pallas as pl
from jax.experimental.pallas import tpu as pltpu
from jax.sharding import PartitionSpec as P

MESH = pl.DeviceIdType.MESH
F32 = jnp.float32
BF = jnp.bfloat16
EPS = 1e-06
LEN = 128
T = 256
NM, G1L, G2L, DL = 256, 1024, 384, 384
FFL = 704
ST = 272


class Event:
    def __init__(self, name, link, size, deps, put, got):
        self.name, self.link, self.size, self.deps = name, link, size, deps
        self.put, self.got = put, got


RATE = {"p": 300.0, "xx": 23.0}
LAT = {"p": 1.0, "xx": 2.6}


def plan(events, tasks):
    done, order, sent, flights = set(), [], set(), []
    free = {}
    now = 0.0

    def launch():
        for e in events:
            if e.name not in sent and all(d in done for d in e.deps):
                sent.add(e.name)
                start = max(now, free.get(e.link, 0.0))
                end = start + e.size / (RATE.get(e.link, 46.0) * 1e3)
                free[e.link] = end
                flights.append((end + LAT.get(e.link, 1.8), e))
                order.append(("send", e))

    launch()
    left = list(tasks)
    while flights or left:
        ready = [t for t in left if all(d in done for d in t[1])]
        landed = [f for f in flights if f[0] <= now]
        if landed:
            f = min(landed, key=lambda v: v[0])
        elif ready:
            t = ready[0]
            left.remove(t)
            order.append(("run", t))
            now += t[2]
            done.add(t[0])
            launch()
            continue
        else:
            f = min(flights, key=lambda v: v[0])
            now = f[0]
        flights.remove(f)
        order.append(("wait", f[1]))
        done.add(f[1].name)
        launch()
    return order


def weight_events(M, G1, G2, D1, D2, W):
    ev = []

    def add(name, link, size, deps, ref):
        ev.append(Event(name, link, size, deps, lambda: ref(*W.shift[link]), lambda: ref(0, 0)))

    def along_z(tag, buf, width, b, have):
        size = 64 * width * 2
        for sign, link in ((-1, "z+"), (1, "z-")):
            add(f"{tag}{link}1", link, size, have, lambda dz, dy, s=sign: buf.at[W.zl(s + dz), W.yy(b + dy)])
        for sign, link, lo in ((-1, "z+", 0), (1, "z-", 32)):
            add(f"{tag}{link}2", link, size // 2, [f"{tag}{link}1"],
                lambda dz, dy, s=sign, lo=lo: buf.at[W.zl(2 * s + dz), W.yy(b + dy), pl.ds(lo, 32)])
        return [f"{tag}z+1", f"{tag}z-1", f"{tag}z+2", f"{tag}z-2"]

    def columns_along_y(tag, buf, width, first):
        names = []
        for s in (1, 2, 3, 4):
            for sign, link, lo in ((-1, "y+", 0), (1, "y-", 2)):
                n, at = (4, 0) if s < 4 else (2, lo)
                add(f"{tag}{link}{s}", link, n * 64 * width * 2, first if s == 1 else [f"{tag}{link}{s - 1}"],
                    lambda dz, dy, s=s, sign=sign, at=at, n=n: buf.at[pl.ds(at, n), W.yy(sign * s + dy)])
                names.append(f"{tag}{link}{s}")
        return names

    def own_along_y(tag, buf, width, first):
        for s in (1, 2, 3, 4):
            for sign, link, lo in ((-1, "y+", 0), (1, "y-", 32)):
                n, at = (64, 0) if s < 4 else (32, lo)
                add(f"{tag}{link}{s}", link, n * width * 2, first if s == 1 else [f"{tag}{link}{s - 1}"],
                    lambda dz, dy, s=s, sign=sign, at=at, n=n: buf.at[W.zl(dz), W.yy(sign * s + dy), pl.ds(at, n)])

    def behind(tag, b):
        if b == 0:
            return []
        if b == 4:
            return [f"{tag}y+4", f"{tag}y-4"]
        return [f"{tag}y+{-b}"] if b < 0 else [f"{tag}y-{b}"]

    mz = along_z("M", M, NM, 0, [])
    all_m = mz + columns_along_y("M", M, NM, mz)
    own_along_y("G", G1, G1L, [])
    g2z = along_z("H", G2, G2L, 0, [])
    all_g = []
    for b in (0, -1, 1, -2, 2, -3, 3, 4):
        all_g += behind("G", b) + along_z(f"G{b}", G1, G1L, b, behind("G", b))
    d1z = along_z("D", D1, DL, 0, [])
    own_along_y("E", D2, DL, ["Gy+2", "Gy-2"])
    all_h = g2z + columns_along_y("H", G2, G2L, g2z + ["My+2", "My-2"])
    d1y = columns_along_y("D", D1, DL, d1z + ["Hy+3", "Hy-3"])
    of_y = {0: list(d1z)}
    for s in (1, 2, 3):
        of_y[-s] = [f"Dy+{s}"]
        of_y[s] = [f"Dy-{s}"]
    of_y[4] = ["Dy+4", "Dy-4"]
    for b in (2, -2, 1, -1, -3, 3, 0, 4):
        late = ["G3z+1", "G3z-1"]
        of_y[b] = of_y[b] + behind("E", b) + along_z(f"E{b}", D2, DL, b, behind("E", b) + late)
    return ev, all_m, all_g, all_h, of_y


class Where:
    pass


def kernel(res_in, mgain_in, cgain_in, v_in, i_in, o_in, w_in, g_in, u_in, d_in,
           vs_in, is_in, os_in, taps_in, cg_in, ms_in, gs_in, us_in, ds_in, out,
           M, G1, G2, D1, D2, X1, X2, XN, hid, keep, own32, preo, prei, rxo, rxi, qo, qi, ro, ri,
           res, mgain, cgain, vw, iw, ow, mw, gw, uw, dw, vs, ivs, ovs, taps, cg, ms, gs, us, ds, small,
           send_sem, recv_sem, loc_sem, n_events):
    rep, fs, tp = lax.axis_index("rep"), lax.axis_index("fs"), lax.axis_index("tp")
    y, zl = lax.rem(fs, 8), lax.div(fs, 8)
    x, c = lax.div(tp, 2), lax.rem(tp, 2)
    z = rep * 4 + zl

    def y_at(d):
        return {"fs": zl * 8 + lax.rem(y + d + 8, 8)}

    def z_at(d):
        zz = lax.rem(z + d + 8, 8)
        return {"rep": lax.div(zz, 4), "fs": lax.rem(zz, 4) * 8 + y}

    def x_at(d):
        return {"tp": lax.rem(x + d + 4, 4) * 2 + c}

    partner = {"tp": x * 2 + 1 - c}
    target = {"y+": y_at(1), "y-": y_at(-1), "z+": z_at(1), "z-": z_at(-1),
              "x+": x_at(1), "x-": x_at(-1), "xx": x_at(2), "p": partner}

    W = Where()
    W.shift = {"y+": (0, 1), "y-": (0, -1), "z+": (1, 0), "z-": (-1, 0)}
    W.zl = lambda d: lax.rem(zl + d + 8, 4)
    W.yy = lambda d: lax.rem(y + d + 16, 8)

    ev, all_m, all_g, all_h, of_y = weight_events(M, G1, G2, D1, D2, W)
    pos = {"x+": -1, "x-": 1, "xx": 2}

    def slot(d, core):
        return lax.rem(x + d + 4, 4) * 2 + core

    def spread(tag, buf, first):
        names = []
        for link in ("x+", "x-", "xx"):
            ev.append(Event(f"{tag}{link}", link, T * 256 * 2, [first] if first else [],
                            lambda: buf.at[slot(0, c)], lambda link=link: buf.at[slot(pos[link], c)]))
            names.append(f"{tag}{link}")
        ev.append(Event(f"{tag}p", "p", T * 256 * 2, [first] if first else [],
                        lambda: buf.at[slot(0, c)], lambda: buf.at[slot(0, 1 - c)]))
        names.append(f"{tag}p")
        for link in ("x+", "x-", "xx"):
            ev.append(Event(f"{tag}p{link}", "p", T * 256 * 2, [f"{tag}{link}"],
                            lambda link=link: buf.at[slot(pos[link], c)],
                            lambda link=link: buf.at[slot(pos[link], 1 - c)]))
            names.append(f"{tag}p{link}")
        return names

    all_x1 = spread("X1", X1, None)
    hop = {"x+": 1, "x-": 3, "xx": 2}
    ev.append(Event("Q", "p", 4 * ST * T * 2, ["mix"], lambda: preo, lambda: prei))
    for link, j in hop.items():
        ev.append(Event(f"R{link}", link, ST * T * 2, ["mixsum"],
                        lambda j=j: rxo.at[j - 1], lambda j=j: rxi.at[j - 1]))
    all_x2 = spread("X2", X2, "after")
    for g in range(4):
        ev.append(Event(f"S{g}", "p", 256 * T * 2, [f"down{g}"], lambda g=g: qo.at[g], lambda g=g: qi.at[g]))
        for link, j in hop.items():
            ev.append(Event(f"U{g}{link}", link, 64 * T * 2, [f"sum{g}"],
                            lambda j=j, g=g: ro.at[g, j - 1], lambda j=j, g=g: ri.at[g, j - 1]))
    assert len(ev) == n_events, len(ev)
    index = {e.name: i for i, e in enumerate(ev)}

    barrier = pltpu.get_barrier_semaphore()
    for dev in target.values():
        pl.semaphore_signal(barrier, inc=1, device_id=dev, device_id_type=MESH)

    ins = [(res_in, res), (v_in, vw), (i_in, iw), (o_in, ow), (w_in, mw), (ms_in, ms), (g_in, gw), (u_in, uw),
           (d_in, dw), (ds_in, ds), (mgain_in, mgain), (cgain_in, cgain), (vs_in, vs), (is_in, ivs), (os_in, ovs),
           (taps_in, taps), (cg_in, cg), (gs_in, gs), (us_in, us)]
    copies = [pltpu.make_async_copy(src, dst, loc_sem.at[i]) for i, (src, dst) in enumerate(ins)]
    for copy in copies:
        copy.start()
    for copy in copies:
        copy.wait()
    half = lax.broadcasted_iota(jnp.int32, (64, 128), 1) < 64
    X1[slot(0, c)] = res[...].astype(F32).T.astype(BF)
    own = (zl, y)
    M[(*own, slice(None), slice(0, 128))] = jnp.concatenate([vw[...], iw[...]], axis=1).astype(BF)
    turned = (mw[...] * ms[...]).T
    M[(*own, slice(None), slice(128, 256))] = jnp.concatenate([ow[...], turned], axis=1).astype(BF)
    for t in range(6):
        if t < 5:
            gate, up = gw[:, 128 * t:128 * t + 128], uw[:, 128 * t:128 * t + 128]
        else:
            gate = jnp.concatenate([gw[:, 640:704]] * 2, axis=1)
            up = jnp.concatenate([uw[:, 640:704]] * 2, axis=1)
        turn = pltpu.roll(up, 64, axis=1)
        pair = [jnp.where(half, gate, turn).astype(BF), jnp.where(half, turn, gate).astype(BF)]
        for k in range(2 if t < 5 else 1):
            n = 2 * t + k
            if n < 8:
                G1[(*own, slice(None), slice(128 * n, 128 * n + 128))] = pair[k]
            else:
                n -= 8
                G2[(*own, slice(None), slice(128 * n, 128 * n + 128))] = pair[k]
    D1[own] = (dw[0:384] * ds[...]).T.astype(BF)
    D2[(*own, slice(None), slice(0, 256))] = (dw[384:640] * ds[...]).T.astype(BF)
    tail = (dw[640:704] * ds[...]).T
    D2[(*own, slice(None), slice(256, 384))] = jnp.concatenate([tail, jnp.zeros((64, 64), F32)], axis=1).astype(BF)
    row = vs[...] * ivs[...] * ovs[...]
    for k in range(3):
        line = taps[k:k + 1] * row
        small[k:k + 1] = jnp.concatenate([line, line], axis=1)
    small[3:4] = jnp.concatenate([cg[...], cg[...]], axis=1)
    pl.semaphore_wait(barrier, 8)

    def start(e):
        i = index[e.name]
        ref = e.put()
        pltpu.make_async_remote_copy(src_ref=ref, dst_ref=ref if e.link[0] in "yz" or e.name[:1] == "X" else e.got(),
                                     send_sem=send_sem.at[i], recv_sem=recv_sem.at[i],
                                     device_id=target[e.link], device_id_type=MESH).start()

    def arrive(e):
        i = index[e.name]
        ref = e.got()
        pltpu.make_async_remote_copy(src_ref=ref, dst_ref=ref, send_sem=send_sem.at[i], recv_sem=recv_sem.at[i],
                                     device_id=target[e.link], device_id_type=MESH).wait_recv()

    def left(e):
        i = index[e.name]
        ref = e.put()
        pltpu.make_async_remote_copy(src_ref=ref, dst_ref=ref, send_sem=send_sem.at[i], recv_sem=recv_sem.at[i],
                                     device_id=target[e.link], device_id_type=MESH).wait_send()

    def normed(buf, gain):
        def square(k, s):
            v = buf[k].astype(F32)
            return s + v * v
        total = lax.fori_loop(0, 8, square, jnp.zeros((T, 256), F32))
        factor = lax.rsqrt(jnp.sum(total, axis=1, keepdims=True) * (1.0 / 2048) + EPS)
        for k in range(8):
            cols = slice(k * 256, k * 256 + 256)
            XN[:, cols] = (buf[k].astype(F32) * factor * gain[0:1, cols]).astype(BF)

    def norm_one():
        normed(X1, mgain)

    def split_stats(s):
        high = s.astype(BF)
        low = (s - high.astype(F32)).astype(BF)
        return jnp.concatenate([high, low], axis=0)

    def mix():
        proj = jnp.dot(XN[...], M[...].reshape(2048, NM), preferred_element_type=F32)
        first, second = proj[:, :128], proj[:, 128:]
        u = first * pltpu.roll(first, 64, axis=1)
        place = lax.rem(lax.broadcasted_iota(jnp.int32, (T, 128), 0), LEN)
        lane = lax.broadcasted_iota(jnp.int32, (T, 128), 1)
        one = jnp.where(place >= 1, pltpu.roll(u, 1, axis=0), 0.0)
        two = jnp.where(place >= 2, pltpu.roll(u, 2, axis=0), 0.0)
        conv = small[2:3] * u + small[1:2] * one + small[0:1] * two
        mixed = jnp.where(lane >= 64, pltpu.roll(second, 64, axis=1) * conv, 0.0)
        sq = mixed * mixed
        high = sq.astype(BF)
        low = (sq - high.astype(F32)).astype(BF)
        ones = jnp.ones((16, 128), BF)
        nt = (((1,), (1,)), ((), ()))
        stat = (lax.dot_general(ones, high, nt, preferred_element_type=F32)
                + lax.dot_general(ones, low, nt, preferred_element_type=F32))[:8]
        scaled = (mixed * small[3:4]).astype(BF)
        for j in range(4):
            for mine in (False, True):
                core = c if mine else 1 - c
                w = M[lax.rem(x + j, 4), pl.ds(4 * core, 4), :, 128:].reshape(256, 128)
                part = lax.dot_general(w, scaled, nt, preferred_element_type=F32)
                if mine:
                    own32[j] = part
                else:
                    preo[j, :256] = part.astype(BF)
                    preo[j, 256:] = split_stats(stat)
        keep[0:8] = stat

    def mixsum():
        stat = keep[0:8] + prei[0, 256:264].astype(F32) + prei[0, 264:272].astype(F32)
        for j in (2, 1, 3):
            rxo[j - 1, :256] = (own32[j] + prei[j, :256].astype(F32)).astype(BF)
            rxo[j - 1, 256:] = split_stats(stat)
        own32[0] = own32[0] + prei[0, :256].astype(F32)
        keep[0:8] = stat

    def after():
        stat = keep[0:8]
        total = own32[0]
        for j in range(3):
            total = total + rxi[j, :256].astype(F32)
            stat = stat + rxi[j, 256:264].astype(F32) + rxi[j, 264:272].astype(F32)
        factor = lax.rsqrt(stat * (1.0 / 512) + EPS)[0:1]
        value = (res[...].astype(F32) + total * factor).astype(BF)
        X2[slot(0, c)] = value.astype(F32).T.astype(BF)
        out[...] = value

    def norm_two():
        normed(X2, cgain)

    lane = lax.broadcasted_iota(jnp.int32, (T, 128), 1)

    def hidden_tiles(w, first, tiles):
        z = jnp.dot(XN[...], w, preferred_element_type=F32)
        for k in range(0, tiles, 2):
            n = (first + k) // 2
            even = z[:, 128 * k:128 * k + 128]
            if k + 1 < tiles:
                odd = z[:, 128 * k + 128:128 * k + 256]
                gsc, usc = gs[0:1, 128 * n:128 * n + 128], us[0:1, 128 * n:128 * n + 128]
            else:
                odd = jnp.zeros((T, 128), F32)
                gsc = jnp.concatenate([gs[0:1, 640:704]] * 2, axis=1)
                usc = jnp.concatenate([us[0:1, 640:704]] * 2, axis=1)
            gate = jnp.where(lane < 64, even, odd) * gsc
            up = pltpu.roll(jnp.where(lane < 64, odd, even), 64, axis=1) * usc
            hid[:, 128 * n:128 * n + 128] = (gate / (1.0 + jnp.exp(-gate)) * up).astype(BF)

    def hidden_one():
        for n in range(4):
            hidden_tiles(G1[:, :, :, n * 256:n * 256 + 256].reshape(2048, 256), 2 * n, 2)

    def hidden_two():
        hidden_tiles(G2[:, :, :, 0:256].reshape(2048, 256), 8, 2)
        hidden_tiles(G2[:, :, :, 256:384].reshape(2048, 128), 10, 1)

    def down(g, core):
        at = lax.rem(y + g, 4) + 4 * core
        nt = (((1,), (1,)), ((), ()))
        p = lax.dot_general(D1[:, at].reshape(256, DL), hid[:, :DL], nt, preferred_element_type=F32)
        q = lax.dot_general(D2[:, at].reshape(256, DL), hid[:, DL:], nt, preferred_element_type=F32)
        return (p + q).reshape(4, 64, T)

    def down_partner(g):
        qo[g] = down(g, 1 - c).astype(BF)

    def down_own(g):
        own32[g] = down(g, c).reshape(256, T)

    def sum_for(g):
        for j in (2, 1, 3):
            x_to = lax.rem(x + j, 4)
            ro[g, j - 1] = (own32[g, pl.ds(pl.multiple_of(x_to * 64, 64), 64)] + qi[g, x_to].astype(F32)).astype(BF)

    def final(g):
        rows = pl.ds(pl.multiple_of(lax.rem(y + g, 4) * 64, 64), 64)
        total = own32[g, pl.ds(pl.multiple_of(x * 64, 64), 64)] + qi[g, x].astype(F32)
        for j in range(3):
            total = total + ri[g, j].astype(F32)
        out[rows] = (out[rows].astype(F32) + total).astype(BF)

    tasks = [
        ("norm1", all_x1, 0.8, norm_one),
        ("mix", ["norm1"] + all_m, 1.5, mix),
        ("mixsum", ["Q"], 0.5, mixsum),
        ("after", ["Rx+", "Rx-", "Rxx"], 0.5, after),
        ("norm2", all_x2, 0.8, norm_two),
        ("hidden1", ["norm2"] + all_g, 1.4, hidden_one),
        ("hidden2", ["norm2"] + all_h, 0.6, hidden_two),
    ]
    for g in (2, 1, 3, 0):
        need = of_y[g] + (of_y[g - 4] if g else of_y[4])
        tasks.append((f"down{g}", ["hidden1", "hidden2"] + need, 0.4, lambda g=g: down_partner(g)))
        tasks.append((f"own{g}", [f"down{g}"], 0.4, lambda g=g: down_own(g)))
        tasks.append((f"sum{g}", [f"own{g}", f"S{g}"], 0.2, lambda g=g: sum_for(g)))
    for g in (2, 1, 3, 0):
        tasks.append((f"final{g}", [f"U{g}x+", f"U{g}x-", f"U{g}xx"], 0.1, lambda g=g: final(g)))
    order = plan(ev, tasks)
    for kind, item in order:
        if kind == "send":
            start(item)
        elif kind == "wait":
            arrive(item)
        else:
            item[3]()
    for e in ev:
        left(e)


N_EVENTS = 12 + 40 + 12 + 12 + 40 + 7 + 1 + 3 + 7 + 4 + 12


def local(residual, mixer_gain, value_weight, value_scale, input_gate_weight, input_gate_scale,
          output_gate_weight, output_gate_scale, conv_taps, conv_gain, mixer_out_weight, mixer_out_scale,
          channel_gain, gate_weight, gate_scale, up_weight, up_scale, down_weight, down_scale):
    def line(a):
        return a.reshape(1, -1)

    hbm = pl.BlockSpec(memory_space=pl.ANY)
    vmem = pl.BlockSpec(memory_space=pltpu.VMEM)
    V = pltpu.VMEM
    return pl.pallas_call(
        functools.partial(kernel, n_events=N_EVENTS),
        out_shape=jax.ShapeDtypeStruct((256, T), BF),
        in_specs=[hbm] * 19,
        out_specs=vmem,
        scratch_shapes=[
            V((4, 8, 64, NM), BF), V((4, 8, 64, G1L), BF), V((4, 8, 64, G2L), BF),
            V((4, 8, 64, DL), BF), V((4, 8, 64, DL), BF),
            V((8, T, 256), BF), V((8, T, 256), BF), V((T, 2048), BF), V((T, 2 * DL), BF),
            V((8, T), F32), V((4, 256, T), F32),
            V((4, ST, T), BF), V((4, ST, T), BF), V((3, ST, T), BF), V((3, ST, T), BF),
            V((4, 4, 64, T), BF), V((4, 4, 64, T), BF), V((4, 3, 64, T), BF), V((4, 3, 64, T), BF),
            V((256, T), BF), V((1, 2048), F32), V((1, 2048), F32), V((64, 64), F32), V((64, 64), F32),
            V((64, 64), F32), V((64, 64), F32), V((64, FFL), F32), V((64, FFL), F32), V((FFL, 64), F32),
            V((1, 64), F32), V((1, 64), F32), V((1, 64), F32), V((3, 64), F32), V((1, 64), F32), V((1, 64), F32),
            V((1, FFL), F32), V((1, FFL), F32), V((1, 64), F32), V((8, 128), F32),
            pltpu.SemaphoreType.DMA((N_EVENTS,)), pltpu.SemaphoreType.DMA((N_EVENTS,)),
            pltpu.SemaphoreType.DMA((19,)),
        ],
        compiler_params=pltpu.CompilerParams(collective_id=0, has_side_effects=True,
                                             vmem_limit_bytes=60 * 1024 * 1024),
        name="layer",
    )(residual, line(mixer_gain), line(channel_gain), value_weight, input_gate_weight, output_gate_weight,
      mixer_out_weight, gate_weight, up_weight, down_weight, line(value_scale), line(input_gate_scale),
      line(output_gate_scale), conv_taps, line(conv_gain), line(mixer_out_scale), line(gate_scale),
      line(up_scale), line(down_scale))


def solution(mesh):
    rf = ("rep", "fs")
    in_specs = (P("tp", rf), P(), P("fs", "tp"), P("tp"), P("fs", "tp"), P("tp"), P("fs", "tp"), P("tp"),
                P(None, "tp"), P("tp"), P("tp", "fs"), P("fs"), P(), P("fs", "tp"), P("tp"), P("fs", "tp"),
                P("tp"), P("tp", "fs"), P("fs"))
    return jax.shard_map(local, mesh=mesh, in_specs=in_specs, out_specs=P("tp", rf), check_vma=False)
```

```python
import functools

import jax
import jax.numpy as jnp
from jax import lax
from jax.experimental import pallas as pl
from jax.experimental.pallas import tpu as pltpu
from jax.sharding import PartitionSpec as P

MESH = pl.DeviceIdType.MESH
F32 = jnp.float32
BF = jnp.bfloat16
EPS = 1e-06
LEN = 128
T = 256
NM, G1L, G2L, D1L, D2L = 256, 1024, 384, 256, 512
FFL = 704
ST = 272


class Event:
    def __init__(self, name, link, size, deps, put, got):
        self.name, self.link, self.size, self.deps = name, link, size, deps
        self.put, self.got = put, got


RATE = {"p": 100.0, "xx": 28.0, "x+": 60.0, "x-": 60.0}
LAT = {"p": 1.5, "xx": 2.6}


def plan(events, tasks):
    done, order, sent, flights = set(), [], set(), []
    passed_on = {d for e in events for d in e.deps}
    by_name = {e.name: e for e in events}
    waited = set()
    free = {}
    now = 0.0

    def launch():
        for e in events:
            if e.name not in sent and all(d in done for d in e.deps):
                sent.add(e.name)
                start = max(now, free.get(e.link, 0.0))
                end = start + e.size / (RATE.get(e.link, 46.0) * 1e3)
                free[e.link] = end
                flights.append((end + LAT.get(e.link, 1.8), e))
                order.append(("send", e))

    launch()
    left = list(tasks)
    while flights or left:
        ready = [t for t in left if all(d in done for d in t[1])]
        landed = [f for f in flights if f[0] <= now]
        if landed:
            f = min(landed, key=lambda v: v[0])
        elif ready:
            t = ready[0]
            left.remove(t)
            for d in t[1]:
                if d in by_name and d not in waited:
                    waited.add(d)
                    order.append(("wait", by_name[d]))
            order.append(("run", t))
            now += t[2]
            done.add(t[0])
            launch()
            continue
        else:
            f = min(flights, key=lambda v: v[0])
            now = f[0]
        flights.remove(f)
        if f[1].name in passed_on:
            waited.add(f[1].name)
            order.append(("wait", f[1]))
        done.add(f[1].name)
        launch()
    return order


def weight_events(M, G1, G2, D1, D2, W):
    ev = []

    def add(name, link, size, deps, ref):
        ev.append(Event(name, link, size, deps, lambda: ref(*W.shift[link]), lambda: ref(0, 0)))

    def along_z(tag, buf, width, b, have):
        size = 64 * width * 2
        for sign, link in ((-1, "z+"), (1, "z-")):
            add(f"{tag}{link}1", link, size, have, lambda dz, dy, s=sign: buf.at[W.zl(s + dz), W.yy(b + dy)])
        for sign, link, lo in ((-1, "z+", 0), (1, "z-", 32)):
            add(f"{tag}{link}2", link, size // 2, [f"{tag}{link}1"],
                lambda dz, dy, s=sign, lo=lo: buf.at[W.zl(2 * s + dz), W.yy(b + dy), pl.ds(lo, 32)])
        return [f"{tag}z+1", f"{tag}z-1", f"{tag}z+2", f"{tag}z-2"]

    def gate(tag, s, link):
        other = GATE.get(f"{tag}{s}")
        return [f"{other[0]}{link}{other[1]}"] if other else []

    def columns_along_y(tag, buf, width, first):
        names = []
        for s in (1, 2, 3, 4):
            for sign, link, lo in ((-1, "y+", 0), (1, "y-", 2)):
                n, at = (4, 0) if s < 4 else (2, lo)
                add(f"{tag}{link}{s}", link, n * 64 * width * 2,
                    (first if s == 1 else [f"{tag}{link}{s - 1}"]) + gate(tag, s, link),
                    lambda dz, dy, s=s, sign=sign, at=at, n=n: buf.at[pl.ds(at, n), W.yy(sign * s + dy)])
                names.append(f"{tag}{link}{s}")
        return names

    def own_along_y(tag, buf, width):
        for s in (1, 2, 3, 4):
            for sign, link, lo in ((-1, "y+", 0), (1, "y-", 32)):
                n, at = (64, 0) if s < 4 else (32, lo)
                add(f"{tag}{link}{s}", link, n * width * 2,
                    ([] if s == 1 else [f"{tag}{link}{s - 1}"]) + gate(tag, s, link),
                    lambda dz, dy, s=s, sign=sign, at=at, n=n: buf.at[W.zl(dz), W.yy(sign * s + dy), pl.ds(at, n)])

    def behind(tag, b):
        if b == 0:
            return []
        if b == 4:
            return [f"{tag}y+4", f"{tag}y-4"]
        return [f"{tag}y+{-b}"] if b < 0 else [f"{tag}y-{b}"]

    def z_names(tag):
        return [f"{tag}z+1", f"{tag}z-1", f"{tag}z+2", f"{tag}z-2"]

    need = {}
    of_y = {0: z_names("D"), 4: ["Dy+4", "Dy-4"]}
    for s in (1, 2, 3):
        of_y[-s] = [f"Dy+{s}"]
        of_y[s] = [f"Dy-{s}"]
    for part in FIRST:
        if part == "M":
            need["M"] = along_z("M", M, NM, 0, []) + columns_along_y("M", M, NM, z_names("M"))
        elif part == "G":
            own_along_y("G", G1, G1L)
        elif part == "E":
            own_along_y("E", D2, D2L)
        elif part == "Hz":
            along_z("H", G2, G2L, 0, [])
        elif part == "Dz":
            along_z("D", D1, D1L, 0, [])
        elif part == "H":
            need["H"] = z_names("H") + columns_along_y("H", G2, G2L, z_names("H"))
        elif part == "D":
            columns_along_y("D", D1, D1L, z_names("D"))
        elif part == "Gz":
            need["G"] = []
            for b in (0, -1, 1, -2, 2, -3, 3, 4):
                need["G"] += behind("G", b) + along_z(f"G{b}", G1, G1L, b, behind("G", b))
        else:
            for b in LAST:
                of_y[b] = of_y[b] + behind("E", b) + along_z(f"E{b}", D2, D2L, b, behind("E", b) + z_names(HOLD)[:2])
    return ev, need["M"], need["G"], need["H"], of_y


FIRST = ("Hz", "M", "H", "E", "Gz", "Dz", "Ez", "G", "D")
LAST = (2, -2, 3, -1, -3, 4, 1, 0)
HOLD = "G4"
GROUPS = (2, 1, 0, 3)
GATE = {
    "H1": "M3", "E2": "G4", "D1": "H1", "M2": "E1", "G3": "G2", "H3": "E2", "D2": "G3", "E3": "E1", "D3":
    "D1", "G4": "G3", "H2": "M4",
}


class Where:
    pass


def kernel(res_in, mgain_in, cgain_in, v_in, i_in, o_in, w_in, g_in, u_in, d_in,
           vs_in, is_in, os_in, taps_in, cg_in, ms_in, gs_in, us_in, ds_in, out,
           M, G1, G2, D1, D2, X1, X2, XN, hid, keep, mixed_to, own32, preo, prei, rxo, rxi, qo, qi, ro, ri,
           res, mgain, cgain, vw, iw, ow, mw, gw, uw, dw, vs, ivs, ovs, taps, cg, ms, gs, us, ds, small,
           send_sem, recv_sem, loc_sem, n_events):
    rep, fs, tp = lax.axis_index("rep"), lax.axis_index("fs"), lax.axis_index("tp")
    y, zl = lax.rem(fs, 8), lax.div(fs, 8)
    x, c = lax.div(tp, 2), lax.rem(tp, 2)
    z = rep * 4 + zl

    def y_at(d):
        return {"fs": zl * 8 + lax.rem(y + d + 8, 8)}

    def z_at(d):
        zz = lax.rem(z + d + 8, 8)
        return {"rep": lax.div(zz, 4), "fs": lax.rem(zz, 4) * 8 + y}

    def x_at(d):
        return {"tp": lax.rem(x + d + 4, 4) * 2 + c}

    partner = {"tp": x * 2 + 1 - c}
    target = {"y+": y_at(1), "y-": y_at(-1), "z+": z_at(1), "z-": z_at(-1),
              "x+": x_at(1), "x-": x_at(-1), "xx": x_at(2), "p": partner}

    W = Where()
    W.shift = {"y+": (0, 1), "y-": (0, -1), "z+": (1, 0), "z-": (-1, 0)}
    W.zl = lambda d: lax.rem(zl + d + 8, 4)
    W.yy = lambda d: lax.rem(y + d + 16, 8)

    ev, all_m, all_g, all_h, of_y = weight_events(M, G1, G2, D1, D2, W)
    pos = {"x+": -1, "x-": 1, "xx": 2}

    def slot(d, core):
        return lax.rem(x + d + 4, 4) * 2 + core

    def spread(tag, buf, first):
        names = []
        for link in ("x+", "x-", "xx"):
            ev.append(Event(f"{tag}{link}", link, T * 256 * 2, [first] if first else [],
                            lambda: buf.at[slot(0, c)], lambda link=link: buf.at[slot(pos[link], c)]))
            names.append(f"{tag}{link}")
        ev.append(Event(f"{tag}p", "p", T * 256 * 2, [first] if first else [],
                        lambda: buf.at[slot(0, c)], lambda: buf.at[slot(0, 1 - c)]))
        names.append(f"{tag}p")
        for link in ("x+", "x-", "xx"):
            ev.append(Event(f"{tag}p{link}", "p", T * 256 * 2, [f"{tag}{link}"],
                            lambda link=link: buf.at[slot(pos[link], c)],
                            lambda link=link: buf.at[slot(pos[link], 1 - c)]))
            names.append(f"{tag}p{link}")
        return names

    all_x1 = spread("X1", X1, None)
    hop = {"x+": 1, "x-": 3, "xx": 2}
    for j in (2, 1, 3, 0):
        ev.append(Event(f"Q{j}", "p", ST * T * 2, [f"mix{j}"], lambda j=j: preo.at[j], lambda j=j: prei.at[j]))
    for link, j in (("xx", 2), ("x+", 1), ("x-", 3)):
        ev.append(Event(f"R{link}", link, ST * T * 2, [f"mixsum{j}"],
                        lambda j=j: rxo.at[j - 1], lambda j=j: rxi.at[j - 1]))
    all_x2 = spread("X2", X2, "after")
    for g in range(4):
        ev.append(Event(f"S{g}", "p", 256 * T * 2, [f"down{g}"], lambda g=g: qo.at[g], lambda g=g: qi.at[g]))
        for link, j in hop.items():
            ev.append(Event(f"U{g}{link}", link, 64 * T * 2, [f"sum{g}"],
                            lambda j=j, g=g: ro.at[g, j - 1], lambda j=j, g=g: ri.at[g, j - 1]))
    assert len(ev) == n_events, len(ev)
    index = {e.name: i for i, e in enumerate(ev)}

    barrier = pltpu.get_barrier_semaphore()
    for dev in target.values():
        pl.semaphore_signal(barrier, inc=1, device_id=dev, device_id_type=MESH)

    ins = [(res_in, res), (v_in, vw), (i_in, iw), (o_in, ow), (w_in, mw), (ms_in, ms), (g_in, gw), (u_in, uw),
           (d_in, dw), (ds_in, ds), (mgain_in, mgain), (cgain_in, cgain), (vs_in, vs), (is_in, ivs), (os_in, ovs),
           (taps_in, taps), (cg_in, cg), (gs_in, gs), (us_in, us)]
    copies = [pltpu.make_async_copy(src, dst, loc_sem.at[i]) for i, (src, dst) in enumerate(ins)]
    for copy in copies:
        copy.start()
    for copy in copies:
        copy.wait()
    half = lax.broadcasted_iota(jnp.int32, (64, 128), 1) < 64
    X1[slot(0, c)] = res[...].astype(F32).T.astype(BF)
    own = (zl, y)
    M[(*own, slice(None), slice(0, 128))] = jnp.concatenate([vw[...], iw[...]], axis=1).astype(BF)
    turned = (mw[...] * ms[...]).T
    M[(*own, slice(None), slice(128, 256))] = jnp.concatenate([ow[...], turned], axis=1).astype(BF)
    for t in range(6):
        if t < 5:
            gate, up = gw[:, 128 * t:128 * t + 128], uw[:, 128 * t:128 * t + 128]
        else:
            gate = jnp.concatenate([gw[:, 640:704]] * 2, axis=1)
            up = jnp.concatenate([uw[:, 640:704]] * 2, axis=1)
        turn = pltpu.roll(up, 64, axis=1)
        pair = [jnp.where(half, gate, turn).astype(BF), jnp.where(half, turn, gate).astype(BF)]
        for k in range(2 if t < 5 else 1):
            n = 2 * t + k
            if n < 8:
                G1[(*own, slice(None), slice(128 * n, 128 * n + 128))] = pair[k]
            else:
                n -= 8
                G2[(*own, slice(None), slice(128 * n, 128 * n + 128))] = pair[k]
    rescale = ds[...].T
    D1[own] = (dw[:, 0:256] * rescale).astype(BF)
    D2[(*own, slice(None), slice(0, 384))] = (dw[:, 256:640] * rescale).astype(BF)
    tail = jnp.concatenate([dw[:, 640:704] * rescale, jnp.zeros((64, 64), F32)], axis=1)
    D2[(*own, slice(None), slice(384, 512))] = tail.astype(BF)
    row = vs[...] * ivs[...] * ovs[...]
    for k in range(3):
        line = taps[k:k + 1] * row
        small[k:k + 1] = jnp.concatenate([line, line], axis=1)
    small[3:4] = jnp.concatenate([cg[...], cg[...]], axis=1)
    pl.semaphore_wait(barrier, 8)

    def start(e):
        i = index[e.name]
        ref = e.put()
        pltpu.make_async_remote_copy(src_ref=ref, dst_ref=ref if e.link[0] in "yz" or e.name[:1] == "X" else e.got(),
                                     send_sem=send_sem.at[i], recv_sem=recv_sem.at[i],
                                     device_id=target[e.link], device_id_type=MESH).start()

    def arrive(e):
        i = index[e.name]
        ref = e.got()
        pltpu.make_async_remote_copy(src_ref=ref, dst_ref=ref, send_sem=send_sem.at[i], recv_sem=recv_sem.at[i],
                                     device_id=target[e.link], device_id_type=MESH).wait_recv()

    def left(e):
        i = index[e.name]
        ref = e.put()
        pltpu.make_async_remote_copy(src_ref=ref, dst_ref=ref, send_sem=send_sem.at[i], recv_sem=recv_sem.at[i],
                                     device_id=target[e.link], device_id_type=MESH).wait_send()

    def normed(buf, gain):
        def square(k, s):
            v = buf[k].astype(F32)
            return s + v * v
        total = lax.fori_loop(0, 8, square, jnp.zeros((T, 256), F32))
        factor = lax.rsqrt(jnp.sum(total, axis=1, keepdims=True) * (1.0 / 2048) + EPS)
        for k in range(8):
            cols = slice(k * 256, k * 256 + 256)
            XN[:, cols] = (buf[k].astype(F32) * factor * gain[0:1, cols]).astype(BF)

    def norm_one():
        normed(X1, mgain)

    def split_stats(s):
        high = s.astype(BF)
        low = (s - high.astype(F32)).astype(BF)
        return jnp.concatenate([high, low], axis=0)

    def mix():
        proj = jnp.dot(XN[...], M[...].reshape(2048, NM), preferred_element_type=F32)
        first, second = proj[:, :128], proj[:, 128:]
        u = first * pltpu.roll(first, 64, axis=1)
        place = lax.rem(lax.broadcasted_iota(jnp.int32, (T, 128), 0), LEN)
        lane = lax.broadcasted_iota(jnp.int32, (T, 128), 1)
        one = jnp.where(place >= 1, pltpu.roll(u, 1, axis=0), 0.0)
        two = jnp.where(place >= 2, pltpu.roll(u, 2, axis=0), 0.0)
        conv = small[2:3] * u + small[1:2] * one + small[0:1] * two
        mixed = jnp.where(lane >= 64, pltpu.roll(second, 64, axis=1) * conv, 0.0)
        sq = mixed * mixed
        high = sq.astype(BF)
        low = (sq - high.astype(F32)).astype(BF)
        ones = jnp.ones((16, 128), BF)
        nt = (((1,), (1,)), ((), ()))
        stat = (lax.dot_general(ones, high, nt, preferred_element_type=F32)
                + lax.dot_general(ones, low, nt, preferred_element_type=F32))[:8]
        scaled = (mixed * small[3:4]).astype(BF)
        mixed_to[...] = scaled
        keep[0:8] = stat

    def mix_for(j):
        nt = (((1,), (1,)), ((), ()))
        for mine in (False, True):
            core = c if mine else 1 - c
            w = M[lax.rem(x + j, 4), pl.ds(4 * core, 4), :, 128:].reshape(256, 128)
            part = lax.dot_general(w, mixed_to[...], nt, preferred_element_type=F32)
            if mine:
                own32[j] = part
            else:
                preo[j, :256] = part.astype(BF)
                preo[j, 256:] = split_stats(keep[0:8])

    def mix_first():
        mix()
        mix_for(2)

    def mixsum(j):
        stat = keep[0:8] + prei[j, 256:264].astype(F32) + prei[j, 264:272].astype(F32)
        rxo[j - 1, :256] = (own32[j] + prei[j, :256].astype(F32)).astype(BF)
        rxo[j - 1, 256:] = split_stats(stat)

    def after():
        stat = keep[0:8] + prei[0, 256:264].astype(F32) + prei[0, 264:272].astype(F32)
        total = own32[0] + prei[0, :256].astype(F32)
        for j in range(3):
            total = total + rxi[j, :256].astype(F32)
            stat = stat + rxi[j, 256:264].astype(F32) + rxi[j, 264:272].astype(F32)
        factor = lax.rsqrt(stat * (1.0 / 512) + EPS)[0:1]
        value = (res[...].astype(F32) + total * factor).astype(BF)
        X2[slot(0, c)] = value.astype(F32).T.astype(BF)
        out[...] = value.astype(F32)

    def norm_two():
        normed(X2, cgain)

    lane = lax.broadcasted_iota(jnp.int32, (T, 128), 1)

    def hidden_tiles(w, first, tiles):
        z = jnp.dot(XN[...], w, preferred_element_type=F32)
        for k in range(0, tiles, 2):
            n = (first + k) // 2
            even = z[:, 128 * k:128 * k + 128]
            if k + 1 < tiles:
                odd = z[:, 128 * k + 128:128 * k + 256]
                gsc, usc = (v[128 * n:128 * n + 128].reshape(1, 128) for v in (gs, us))
            else:
                odd = jnp.zeros((T, 128), F32)
                gsc = jnp.concatenate([gs[640:704].reshape(1, 64)] * 2, axis=1)
                usc = jnp.concatenate([us[640:704].reshape(1, 64)] * 2, axis=1)
            gate = jnp.where(lane < 64, even, odd) * gsc
            up = pltpu.roll(jnp.where(lane < 64, odd, even), 64, axis=1) * usc
            hid[:, 128 * n:128 * n + 128] = (gate / (1.0 + jnp.exp(-gate)) * up).astype(BF)

    def hidden_one():
        for n in range(4):
            hidden_tiles(G1[:, :, :, n * 256:n * 256 + 256].reshape(2048, 256), 2 * n, 2)

    def hidden_two():
        hidden_tiles(G2[:, :, :, 0:256].reshape(2048, 256), 8, 2)
        hidden_tiles(G2[:, :, :, 256:384].reshape(2048, 128), 10, 1)

    def down(g, core):
        at = lax.rem(y + g, 4) + 4 * core
        nt = (((1,), (1,)), ((), ()))
        p = lax.dot_general(D1[:, at].reshape(256, D1L), hid[:, :D1L], nt, preferred_element_type=F32)
        q = lax.dot_general(D2[:, at].reshape(256, D2L), hid[:, D1L:], nt, preferred_element_type=F32)
        return (p + q).reshape(4, 64, T)

    def down_partner(g):
        qo[g] = down(g, 1 - c).astype(BF)

    def down_own(g):
        own32[g] = down(g, c).reshape(256, T)

    def sum_for(g):
        for j in (2, 1, 3):
            x_to = lax.rem(x + j, 4)
            ro[g, j - 1] = (own32[g, pl.ds(pl.multiple_of(x_to * 64, 64), 64)] + qi[g, x_to].astype(F32)).astype(BF)

    def final(g):
        rows = pl.ds(pl.multiple_of(lax.rem(y + g, 4) * 64, 64), 64)
        total = own32[g, pl.ds(pl.multiple_of(x * 64, 64), 64)] + qi[g, x].astype(F32)
        for j in range(3):
            total = total + ri[g, j].astype(F32)
        out[rows] = out[rows] + total

    tasks = [
        ("norm1", all_x1, 0.8, norm_one),
        ("mix2", ["norm1"] + all_m, 1.0, mix_first),
        ("mix1", ["mix2"], 0.2, lambda: mix_for(1)),
        ("mix3", ["mix1"], 0.2, lambda: mix_for(3)),
        ("mix0", ["mix3"], 0.2, lambda: mix_for(0)),
        ("mixsum2", ["Q2", "mix0"], 0.05, lambda: mixsum(2)),
        ("mixsum1", ["Q1", "mix0"], 0.05, lambda: mixsum(1)),
        ("mixsum3", ["Q3", "mix0"], 0.05, lambda: mixsum(3)),
        ("after", ["Q0", "mixsum2", "mixsum1", "mixsum3", "Rx+", "Rx-", "Rxx"], 0.2, after),
        ("norm2", all_x2, 0.8, norm_two),
        ("hidden1", ["norm2"] + all_g, 1.4, hidden_one),
        ("hidden2", ["norm2"] + all_h, 0.8, hidden_two),
    ]
    for g in GROUPS:
        need = of_y[g] + (of_y[g - 4] if g else of_y[4])
        tasks.append((f"down{g}", ["hidden1", "hidden2"] + need, 0.4, lambda g=g: down_partner(g)))
        tasks.append((f"own{g}", [f"down{g}"], 0.4, lambda g=g: down_own(g)))
        tasks.append((f"sum{g}", [f"own{g}", f"S{g}"], 0.2, lambda g=g: sum_for(g)))
    for g in GROUPS:
        tasks.append((f"final{g}", [f"U{g}x+", f"U{g}x-", f"U{g}xx"], 0.1, lambda g=g: final(g)))
    order = plan(ev, tasks)
    for kind, item in order:
        if kind == "send":
            start(item)
        elif kind == "wait":
            arrive(item)
        else:
            item[3]()
    for e in ev:
        left(e)


N_EVENTS = 12 + 40 + 12 + 12 + 40 + 7 + 4 + 3 + 7 + 4 + 12


def local(residual, mixer_gain, value_weight, value_scale, input_gate_weight, input_gate_scale,
          output_gate_weight, output_gate_scale, conv_taps, conv_gain, mixer_out_weight, mixer_out_scale,
          channel_gain, gate_weight, gate_scale, up_weight, up_scale, down_weight, down_scale):
    def line(a):
        return a.reshape(1, -1)

    hbm = pl.BlockSpec(memory_space=pl.ANY)
    vmem = pl.BlockSpec(memory_space=pltpu.VMEM)
    V = pltpu.VMEM
    return pl.pallas_call(
        functools.partial(kernel, n_events=N_EVENTS),
        out_shape=jax.ShapeDtypeStruct((256, T), F32),
        in_specs=[hbm] * 19,
        out_specs=vmem,
        scratch_shapes=[
            V((4, 8, 64, NM), BF), V((4, 8, 64, G1L), BF), V((4, 8, 64, G2L), BF),
            V((4, 8, 64, D1L), BF), V((4, 8, 64, D2L), BF),
            V((8, T, 256), BF), V((8, T, 256), BF), V((T, 2048), BF), V((T, D1L + D2L), BF),
            V((8, T), F32), V((T, 128), BF), V((4, 256, T), F32),
            V((4, ST, T), BF), V((4, ST, T), BF), V((3, ST, T), BF), V((3, ST, T), BF),
            V((4, 4, 64, T), BF), V((4, 4, 64, T), BF), V((4, 3, 64, T), BF), V((4, 3, 64, T), BF),
            V((256, T), BF), V((1, 2048), F32), V((1, 2048), F32), V((64, 64), F32), V((64, 64), F32),
            V((64, 64), F32), V((64, 64), F32), V((64, FFL), F32), V((64, FFL), F32), V((64, FFL), F32),
            V((1, 64), F32), V((1, 64), F32), V((1, 64), F32), V((3, 64), F32), V((1, 64), F32), V((1, 64), F32),
            V((FFL,), F32), V((FFL,), F32), V((1, 64), F32), V((8, 128), F32),
            pltpu.SemaphoreType.DMA((N_EVENTS,)), pltpu.SemaphoreType.DMA((N_EVENTS,)),
            pltpu.SemaphoreType.DMA((19,)),
        ],
        compiler_params=pltpu.CompilerParams(collective_id=0, has_side_effects=True,
                                             vmem_limit_bytes=60 * 1024 * 1024),
        name="layer",
    )(residual, line(mixer_gain), line(channel_gain), value_weight, input_gate_weight, output_gate_weight,
      mixer_out_weight, gate_weight, up_weight, down_weight.T, line(value_scale), line(input_gate_scale),
      line(output_gate_scale), conv_taps, line(conv_gain), line(mixer_out_scale), gate_scale,
      up_scale, line(down_scale)).astype(BF)


def solution(mesh):
    rf = ("rep", "fs")
    in_specs = (P("tp", rf), P(), P("fs", "tp"), P("tp"), P("fs", "tp"), P("tp"), P("fs", "tp"), P("tp"),
                P(None, "tp"), P("tp"), P("tp", "fs"), P("fs"), P(), P("fs", "tp"), P("tp"), P("fs", "tp"),
                P("tp"), P("tp", "fs"), P("fs"))
    return jax.shard_map(local, mesh=mesh, in_specs=in_specs, out_specs=P("tp", rf), check_vma=False)
```

```python
import functools

import jax
import jax.numpy as jnp
from jax import lax
from jax.experimental import pallas as pl
from jax.experimental.pallas import tpu as pltpu
from jax.sharding import PartitionSpec as P

MESH = pl.DeviceIdType.MESH
F32 = jnp.float32
BF = jnp.bfloat16
EPS = 1e-06
LEN = 128
T = 256
NM, G1L, G2L, D1L, D2L = 256, 1024, 384, 256, 512
FFL = 704
ST = 272


class Event:
    def __init__(self, name, link, size, deps, put, got):
        self.name, self.link, self.size, self.deps = name, link, size, deps
        self.put, self.got = put, got


RATE = {"p": 100.0, "xx": 28.0, "x+": 60.0, "x-": 60.0}
LAT = {"p": 1.5, "xx": 2.6}


def landing(name):
    kind, last = name[0], name[-1]
    if kind == "G" and "z" in name and last == "2":
        return "Gz2"
    if kind == "E" and "z" in name and last == "2":
        return f"Ez2{int(name[1:name.index('z')]) % 4}"
    if kind in "MHD" and "y" in name and last == "4":
        return kind + "y4"
    if kind == "X" and name[2] == "p":
        return name[:3]
    if kind in "RU":
        return name[:1 if kind == "R" else 2]
    return name


def leaving(name):
    if name[0] in "XQRSU":
        return name[:2] if name[0] == "X" else name[0]
    return name[0] + ("z" if "z" in name else "y")


def plan(events, tasks):
    done, order, sent, flights = set(), [], set(), []
    passed_on = {d for e in events for d in e.deps}
    by_name = {e.name: e for e in events}
    waited = set()
    free = {}
    now = 0.0

    def launch():
        for e in events:
            if e.name not in sent and all(d in done for d in e.deps):
                sent.add(e.name)
                start = max(now, free.get(e.link, 0.0))
                end = start + e.size / (RATE.get(e.link, 46.0) * 1e3)
                free[e.link] = end
                flights.append((end + LAT.get(e.link, 1.8), e))
                order.append(("send", e))

    launch()
    left = list(tasks)
    while flights or left:
        ready = [t for t in left if all(d in done for d in t[1])]
        landed = [f for f in flights if f[0] <= now]
        if landed:
            f = min(landed, key=lambda v: v[0])
        elif ready:
            t = ready[0]
            left.remove(t)
            for d in t[1]:
                if d in by_name and landing(d) not in waited:
                    waited.add(landing(d))
                    order.append(("wait", by_name[d]))
            order.append(("run", t))
            now += t[2]
            done.add(t[0])
            launch()
            continue
        else:
            f = min(flights, key=lambda v: v[0])
            now = f[0]
        flights.remove(f)
        if f[1].name in passed_on and landing(f[1].name) not in waited:
            waited.add(landing(f[1].name))
            order.append(("wait", f[1]))
        done.add(f[1].name)
        launch()
    return order


def weight_events(M, G1, G2, D1, D2, W):
    ev = []

    def add(name, link, size, deps, ref):
        ev.append(Event(name, link, size, deps, lambda: ref(*W.shift[link]), lambda: ref(0, 0)))

    def along_z(tag, buf, width, b, have):
        have = have or CAST.get(tag[0], [])
        size = 64 * width * 2
        for sign, link in ((-1, "z+"), (1, "z-")):
            add(f"{tag}{link}1", link, size, have, lambda dz, dy, s=sign: buf.at[W.zl(s + dz), W.yy(b + dy)])
        for sign, link, lo in ((-1, "z+", 0), (1, "z-", 32)):
            add(f"{tag}{link}2", link, size // 2, [f"{tag}{link}1"],
                lambda dz, dy, s=sign, lo=lo: buf.at[W.zl(2 * s + dz), W.yy(b + dy), pl.ds(lo, 32)])
        return [f"{tag}z+1", f"{tag}z-1", f"{tag}z+2", f"{tag}z-2"]

    def gate(tag, s, link):
        other = GATE.get(f"{tag}{s}")
        return [f"{other[0]}{link}{other[1]}"] if other else []

    def columns_along_y(tag, buf, width, first):
        names = []
        for s in (1, 2, 3, 4):
            for sign, link, lo in ((-1, "y+", 0), (1, "y-", 2)):
                n, at = (4, 0) if s < 4 else (2, lo)
                add(f"{tag}{link}{s}", link, n * 64 * width * 2,
                    (first if s == 1 else [f"{tag}{link}{s - 1}"]) + gate(tag, s, link),
                    lambda dz, dy, s=s, sign=sign, at=at, n=n: buf.at[pl.ds(at, n), W.yy(sign * s + dy)])
                names.append(f"{tag}{link}{s}")
        return names

    def own_along_y(tag, buf, width):
        for s in (1, 2, 3, 4):
            for sign, link, lo in ((-1, "y+", 0), (1, "y-", 32)):
                n, at = (64, 0) if s < 4 else (32, lo)
                add(f"{tag}{link}{s}", link, n * width * 2,
                    (CAST[tag] if s == 1 else [f"{tag}{link}{s - 1}"]) + gate(tag, s, link),
                    lambda dz, dy, s=s, sign=sign, at=at, n=n: buf.at[W.zl(dz), W.yy(sign * s + dy), pl.ds(at, n)])

    def behind(tag, b):
        if b == 0:
            return []
        if b == 4:
            return [f"{tag}y+4", f"{tag}y-4"]
        return [f"{tag}y+{-b}"] if b < 0 else [f"{tag}y-{b}"]

    def z_names(tag):
        return [f"{tag}z+1", f"{tag}z-1", f"{tag}z+2", f"{tag}z-2"]

    need = {}
    of_y = {0: z_names("D"), 4: ["Dy+4", "Dy-4"]}
    for s in (1, 2, 3):
        of_y[-s] = [f"Dy+{s}"]
        of_y[s] = [f"Dy-{s}"]
    for part in FIRST:
        if part == "M":
            need["M"] = along_z("M", M, NM, 0, []) + columns_along_y("M", M, NM, z_names("M"))
        elif part == "G":
            own_along_y("G", G1, G1L)
        elif part == "E":
            own_along_y("E", D2, D2L)
        elif part == "Hz":
            along_z("H", G2, G2L, 0, [])
        elif part == "Dz":
            along_z("D", D1, D1L, 0, [])
        elif part == "H":
            need["H"] = z_names("H") + columns_along_y("H", G2, G2L, z_names("H"))
        elif part == "D":
            columns_along_y("D", D1, D1L, z_names("D"))
        elif part == "Gz":
            need["G"] = []
            for b in (0, -1, 1, -2, 2, -3, 3, 4):
                need["G"] += behind("G", b) + along_z(f"G{b}", G1, G1L, b, behind("G", b))
        else:
            for b in LAST:
                of_y[b] = of_y[b] + behind("E", b) + along_z(f"E{b}", D2, D2L, b, CAST["E"] + behind("E", b) + z_names(HOLD)[:2])
    return ev, need["M"], need["G"], need["H"], of_y


CAST = {"G": ["castG"], "H": ["castG"], "D": ["castD"], "E": ["castD"]}
FIRST = ("Hz", "M", "H", "E", "Gz", "Dz", "Ez", "G", "D")
LAST = (2, -2, 3, -1, -3, 4, 1, 0)
HOLD = "G4"
GROUPS = (2, 1, 0, 3)
GATE = {
    "H1": "M3", "E2": "G4", "D1": "H1", "M2": "E1", "G3": "G2", "H3": "E2", "D2": "G3", "E3": "E1", "D3":
    "D1", "G4": "G3", "H2": "M4",
}


class Where:
    pass


def kernel(res_in, mgain_in, cgain_in, v_in, i_in, o_in, w_in, g_in, u_in, d_in,
           vs_in, is_in, os_in, taps_in, cg_in, ms_in, gs_in, us_in, ds_in, out,
           M, G1, G2, D1, D2, X1, X2, XN, hid, keep, mixed_to, own32, preo, prei, rxo, rxi, qo, qi, ro, ri,
           res, mgain, cgain, vw, iw, ow, mw, gw, uw, dw, vs, ivs, ovs, taps, cg, ms, gs, us, ds, small,
           send_sem, recv_sem, loc_sem, n_events):
    rep, fs, tp = lax.axis_index("rep"), lax.axis_index("fs"), lax.axis_index("tp")
    y, zl = lax.rem(fs, 8), lax.div(fs, 8)
    x, c = lax.div(tp, 2), lax.rem(tp, 2)
    z = rep * 4 + zl

    def y_at(d):
        return {"fs": zl * 8 + lax.rem(y + d + 8, 8)}

    def z_at(d):
        zz = lax.rem(z + d + 8, 8)
        return {"rep": lax.div(zz, 4), "fs": lax.rem(zz, 4) * 8 + y}

    def x_at(d):
        return {"tp": lax.rem(x + d + 4, 4) * 2 + c}

    partner = {"tp": x * 2 + 1 - c}
    target = {"y+": y_at(1), "y-": y_at(-1), "z+": z_at(1), "z-": z_at(-1),
              "x+": x_at(1), "x-": x_at(-1), "xx": x_at(2), "p": partner}

    W = Where()
    W.shift = {"y+": (0, 1), "y-": (0, -1), "z+": (1, 0), "z-": (-1, 0)}
    W.zl = lambda d: lax.rem(zl + d + 8, 4)
    W.yy = lambda d: lax.rem(y + d + 16, 8)

    ev, all_m, all_g, all_h, of_y = weight_events(M, G1, G2, D1, D2, W)
    pos = {"x+": -1, "x-": 1, "xx": 2}

    def slot(d, core):
        return lax.rem(x + d + 4, 4) * 2 + core

    def spread(tag, buf, first):
        names = []
        for link in ("x+", "x-", "xx"):
            ev.append(Event(f"{tag}{link}", link, T * 256 * 2, [first] if first else [],
                            lambda: buf.at[slot(0, c)], lambda link=link: buf.at[slot(pos[link], c)]))
            names.append(f"{tag}{link}")
        ev.append(Event(f"{tag}p", "p", T * 256 * 2, [first] if first else [],
                        lambda: buf.at[slot(0, c)], lambda: buf.at[slot(0, 1 - c)]))
        names.append(f"{tag}p")
        for link in ("x+", "x-", "xx"):
            ev.append(Event(f"{tag}p{link}", "p", T * 256 * 2, [f"{tag}{link}"],
                            lambda link=link: buf.at[slot(pos[link], c)],
                            lambda link=link: buf.at[slot(pos[link], 1 - c)]))
            names.append(f"{tag}p{link}")
        return names

    all_x1 = spread("X1", X1, None)
    hop = {"x+": 1, "x-": 3, "xx": 2}
    for j in (2, 1, 3, 0):
        ev.append(Event(f"Q{j}", "p", ST * T * 2, [f"mix{j}"], lambda j=j: preo.at[j], lambda j=j: prei.at[j]))
    for link, j in (("xx", 2), ("x+", 1), ("x-", 3)):
        ev.append(Event(f"R{link}", link, ST * T * 2, [f"mixsum{j}"],
                        lambda j=j: rxo.at[j - 1], lambda j=j: rxi.at[j - 1]))
    all_x2 = spread("X2", X2, "after")
    for g in range(4):
        ev.append(Event(f"S{g}", "p", 256 * T * 2, [f"down{g}"], lambda g=g: qo.at[g], lambda g=g: qi.at[g]))
        for link, j in hop.items():
            ev.append(Event(f"U{g}{link}", link, 64 * T * 2, [f"sum{g}"],
                            lambda j=j, g=g: ro.at[g, j - 1], lambda j=j, g=g: ri.at[g, j - 1]))
    assert len(ev) == n_events, len(ev)

    barrier = pltpu.get_barrier_semaphore()
    for dev in target.values():
        pl.semaphore_signal(barrier, inc=1, device_id=dev, device_id_type=MESH)

    ins = [(res_in, res), (v_in, vw), (i_in, iw), (o_in, ow), (w_in, mw), (ms_in, ms), (g_in, gw), (u_in, uw),
           (d_in, dw), (ds_in, ds), (mgain_in, mgain), (cgain_in, cgain), (vs_in, vs), (is_in, ivs), (os_in, ovs),
           (taps_in, taps), (cg_in, cg), (gs_in, gs), (us_in, us)]
    copies = [pltpu.make_async_copy(src, dst, loc_sem.at[i]) for i, (src, dst) in enumerate(ins)]
    for copy in copies:
        copy.start()
    def ready(*which):
        for i in which:
            copies[i].wait()

    own = (zl, y)
    ready(0, 1, 2, 3, 4, 5)
    X1[slot(0, c)] = res[...].astype(F32).T.astype(BF)
    M[(*own, slice(None), slice(0, 128))] = jnp.concatenate([vw[...], iw[...]], axis=1).astype(BF)
    turned = (mw[...] * ms[...]).T
    M[(*own, slice(None), slice(128, 256))] = jnp.concatenate([ow[...], turned], axis=1).astype(BF)

    def cast_gate_up():
        ready(6, 7)
        half = lax.broadcasted_iota(jnp.int32, (64, 128), 1) < 64
        for t in range(6):
            if t < 5:
                gate, up = gw[:, 128 * t:128 * t + 128], uw[:, 128 * t:128 * t + 128]
            else:
                gate = jnp.concatenate([gw[:, 640:704]] * 2, axis=1)
                up = jnp.concatenate([uw[:, 640:704]] * 2, axis=1)
            turn = pltpu.roll(up, 64, axis=1)
            pair = [jnp.where(half, gate, turn).astype(BF), jnp.where(half, turn, gate).astype(BF)]
            for k in range(2 if t < 5 else 1):
                n = 2 * t + k
                if n < G1L // 128:
                    G1[(*own, slice(None), slice(128 * n, 128 * n + 128))] = pair[k]
                else:
                    n -= G1L // 128
                    G2[(*own, slice(None), slice(128 * n, 128 * n + 128))] = pair[k]

    def cast_down():
        ready(8, 9)
        rescale = ds[...].T
        D1[own] = (dw[:, 0:256] * rescale).astype(BF)
        D2[(*own, slice(None), slice(0, 384))] = (dw[:, 256:640] * rescale).astype(BF)
        tail = jnp.concatenate([dw[:, 640:704] * rescale, jnp.zeros((64, 64), F32)], axis=1)
        D2[(*own, slice(None), slice(384, 512))] = tail.astype(BF)
        ready(*range(10, 19))
        row = vs[...] * ivs[...] * ovs[...]
        for k in range(3):
            line = taps[k:k + 1] * row
            small[k:k + 1] = jnp.concatenate([line, line], axis=1)
        small[3:4] = jnp.concatenate([cg[...], cg[...]], axis=1)

    pl.semaphore_wait(barrier, 8)

    bufs = {"M": M, "G": G1, "H": G2, "D": D1, "E": D2}
    out_total = {"X1": X1.at[:7], "X2": X2.at[:7], "Q": preo, "R": rxo, "S": qo, "U": ro}
    in_total = {"Gz2": G1.at[0], "X1p": X1.at[:4], "X2p": X2.at[:4], "R": rxi}
    for k, buf in bufs.items():
        if k in "MHD":
            out_total[k + "z"], out_total[k + "y"] = buf.at[0, :3], buf.at[:, :7]
            in_total[k + "y4"] = buf.at[:, 0]
        else:
            out_total[k + "z"], out_total[k + "y"] = buf.at[:3], buf.at[0, :7]
    for g in range(4):
        in_total[f"Ez2{g}"] = D2.at[0, :2]
        in_total[f"U{g}"] = ri.at[g]
    out_index = {k: i for i, k in enumerate(out_total)}
    in_index = {k: i for i, k in enumerate(dict.fromkeys(landing(e.name) for e in ev))}
    assert len(out_index) == N_OUT and len(in_index) == N_IN, (len(out_index), len(in_index))

    def start(e):
        ref = e.put()
        pltpu.make_async_remote_copy(
            src_ref=ref, dst_ref=ref if e.link[0] in "yz" or e.name[:1] == "X" else e.got(),
            send_sem=send_sem.at[out_index[leaving(e.name)]], recv_sem=recv_sem.at[in_index[landing(e.name)]],
            device_id=target[e.link], device_id_type=MESH).start()

    def arrive(e):
        key = landing(e.name)
        ref = in_total[key] if key in in_total else e.got()
        pltpu.make_async_remote_copy(src_ref=ref, dst_ref=ref, send_sem=send_sem.at[0],
                                     recv_sem=recv_sem.at[in_index[key]],
                                     device_id=target[e.link], device_id_type=MESH).wait_recv()

    def left():
        for key, i in out_index.items():
            ref = out_total[key]
            pltpu.make_async_remote_copy(src_ref=ref, dst_ref=ref, send_sem=send_sem.at[i], recv_sem=recv_sem.at[0],
                                         device_id=partner, device_id_type=MESH).wait_send()

    def normed(buf, gain):
        def square(k, s):
            v = buf[k].astype(F32)
            return s + v * v
        total = lax.fori_loop(0, 8, square, jnp.zeros((T, 256), F32))
        factor = lax.rsqrt(jnp.sum(total, axis=1, keepdims=True) * (1.0 / 2048) + EPS)
        for k in range(8):
            cols = slice(k * 256, k * 256 + 256)
            XN[:, cols] = (buf[k].astype(F32) * factor * gain[0:1, cols]).astype(BF)

    def norm_one():
        normed(X1, mgain)

    def split_stats(s):
        high = s.astype(BF)
        low = (s - high.astype(F32)).astype(BF)
        return jnp.concatenate([high, low], axis=0)

    def mix():
        proj = jnp.dot(XN[...], M[...].reshape(2048, NM), preferred_element_type=F32)
        first, second = proj[:, :128], proj[:, 128:]
        u = first * pltpu.roll(first, 64, axis=1)
        place = lax.rem(lax.broadcasted_iota(jnp.int32, (T, 128), 0), LEN)
        lane = lax.broadcasted_iota(jnp.int32, (T, 128), 1)
        one = jnp.where(place >= 1, pltpu.roll(u, 1, axis=0), 0.0)
        two = jnp.where(place >= 2, pltpu.roll(u, 2, axis=0), 0.0)
        conv = small[2:3] * u + small[1:2] * one + small[0:1] * two
        mixed = jnp.where(lane >= 64, pltpu.roll(second, 64, axis=1) * conv, 0.0)
        sq = mixed * mixed
        high = sq.astype(BF)
        low = (sq - high.astype(F32)).astype(BF)
        ones = jnp.ones((16, 128), BF)
        nt = (((1,), (1,)), ((), ()))
        stat = (lax.dot_general(ones, high, nt, preferred_element_type=F32)
                + lax.dot_general(ones, low, nt, preferred_element_type=F32))[:8]
        scaled = (mixed * small[3:4]).astype(BF)
        mixed_to[...] = scaled
        keep[0:8] = stat

    def mix_for(j):
        nt = (((1,), (1,)), ((), ()))
        for mine in (False, True):
            core = c if mine else 1 - c
            w = M[lax.rem(x + j, 4), pl.ds(4 * core, 4), :, 128:].reshape(256, 128)
            part = lax.dot_general(w, mixed_to[...], nt, preferred_element_type=F32)
            if mine:
                own32[j] = part
            else:
                preo[j, :256] = part.astype(BF)
                preo[j, 256:] = split_stats(keep[0:8])

    def mix_first():
        mix()
        mix_for(2)

    def mixsum(j):
        stat = keep[0:8] + prei[j, 256:264].astype(F32) + prei[j, 264:272].astype(F32)
        rxo[j - 1, :256] = (own32[j] + prei[j, :256].astype(F32)).astype(BF)
        rxo[j - 1, 256:] = split_stats(stat)

    def after():
        stat = keep[0:8] + prei[0, 256:264].astype(F32) + prei[0, 264:272].astype(F32)
        total = own32[0] + prei[0, :256].astype(F32)
        for j in range(3):
            total = total + rxi[j, :256].astype(F32)
            stat = stat + rxi[j, 256:264].astype(F32) + rxi[j, 264:272].astype(F32)
        factor = lax.rsqrt(stat * (1.0 / 512) + EPS)[0:1]
        value = (res[...].astype(F32) + total * factor).astype(BF)
        X2[slot(0, c)] = value.astype(F32).T.astype(BF)
        out[...] = value.astype(F32)

    def norm_two():
        normed(X2, cgain)

    lane = lax.broadcasted_iota(jnp.int32, (T, 128), 1)

    def hidden_tiles(w, first, tiles):
        z = jnp.dot(XN[...], w, preferred_element_type=F32)
        for k in range(0, tiles, 2):
            n = (first + k) // 2
            even = z[:, 128 * k:128 * k + 128]
            if k + 1 < tiles:
                odd = z[:, 128 * k + 128:128 * k + 256]
                gsc, usc = (v[128 * n:128 * n + 128].reshape(1, 128) for v in (gs, us))
            else:
                odd = jnp.zeros((T, 128), F32)
                gsc = jnp.concatenate([gs[640:704].reshape(1, 64)] * 2, axis=1)
                usc = jnp.concatenate([us[640:704].reshape(1, 64)] * 2, axis=1)
            gate = jnp.where(lane < 64, even, odd) * gsc
            up = pltpu.roll(jnp.where(lane < 64, odd, even), 64, axis=1) * usc
            hid[:, 128 * n:128 * n + 128] = (gate / (1.0 + jnp.exp(-gate)) * up).astype(BF)

    def hidden_one():
        for n in range(4):
            hidden_tiles(G1[:, :, :, n * 256:n * 256 + 256].reshape(2048, 256), 2 * n, 2)

    def hidden_two():
        hidden_tiles(G2[:, :, :, 0:256].reshape(2048, 256), 8, 2)
        hidden_tiles(G2[:, :, :, 256:384].reshape(2048, 128), 10, 1)

    def down(g, core):
        at = lax.rem(y + g, 4) + 4 * core
        nt = (((1,), (1,)), ((), ()))
        p = lax.dot_general(D1[:, at].reshape(256, D1L), hid[:, :D1L], nt, preferred_element_type=F32)
        q = lax.dot_general(D2[:, at].reshape(256, D2L), hid[:, D1L:], nt, preferred_element_type=F32)
        return (p + q).reshape(4, 64, T)

    def down_partner(g):
        qo[g] = down(g, 1 - c).astype(BF)

    def down_own(g):
        own32[g] = down(g, c).reshape(256, T)

    def sum_for(g):
        for j in (2, 1, 3):
            x_to = lax.rem(x + j, 4)
            ro[g, j - 1] = (own32[g, pl.ds(pl.multiple_of(x_to * 64, 64), 64)] + qi[g, x_to].astype(F32)).astype(BF)

    def final(g):
        rows = pl.ds(pl.multiple_of(lax.rem(y + g, 4) * 64, 64), 64)
        total = own32[g, pl.ds(pl.multiple_of(x * 64, 64), 64)] + qi[g, x].astype(F32)
        for j in range(3):
            total = total + ri[g, j].astype(F32)
        out[rows] = out[rows] + total

    tasks = [
        ("castG", [], 0.4, cast_gate_up),
        ("castD", ["castG"], 0.4, cast_down),
        ("norm1", all_x1, 0.8, norm_one),
        ("mix2", ["norm1"] + all_m, 1.0, mix_first),
        ("mix1", ["mix2"], 0.2, lambda: mix_for(1)),
        ("mix3", ["mix1"], 0.2, lambda: mix_for(3)),
        ("mix0", ["mix3"], 0.2, lambda: mix_for(0)),
        ("mixsum2", ["Q2", "mix0"], 0.05, lambda: mixsum(2)),
        ("mixsum1", ["Q1", "mix0"], 0.05, lambda: mixsum(1)),
        ("mixsum3", ["Q3", "mix0"], 0.05, lambda: mixsum(3)),
        ("after", ["Q0", "mixsum2", "mixsum1", "mixsum3", "Rx+", "Rx-", "Rxx"], 0.2, after),
        ("norm2", all_x2, 0.8, norm_two),
        ("hidden1", ["norm2"] + all_g, 1.4, hidden_one),
        ("hidden2", ["norm2"] + all_h, 0.8, hidden_two),
    ]
    for g in GROUPS:
        need = of_y[g] + (of_y[g - 4] if g else of_y[4])
        tasks.append((f"down{g}", ["hidden1", "hidden2"] + need, 0.4, lambda g=g: down_partner(g)))
        tasks.append((f"own{g}", [f"down{g}"], 0.4, lambda g=g: down_own(g)))
        tasks.append((f"sum{g}", [f"own{g}", f"S{g}"], 0.2, lambda g=g: sum_for(g)))
    for g in GROUPS:
        tasks.append((f"final{g}", [f"U{g}x+", f"U{g}x-", f"U{g}xx"], 0.1, lambda g=g: final(g)))
    order = plan(ev, tasks)
    for kind, item in order:
        if kind == "send":
            start(item)
        elif kind == "wait":
            arrive(item)
        else:
            item[3]()
    left()


N_EVENTS = 12 + 40 + 12 + 12 + 40 + 7 + 4 + 3 + 7 + 4 + 12
N_OUT, N_IN = 16, 107


def local(residual, mixer_gain, value_weight, value_scale, input_gate_weight, input_gate_scale,
          output_gate_weight, output_gate_scale, conv_taps, conv_gain, mixer_out_weight, mixer_out_scale,
          channel_gain, gate_weight, gate_scale, up_weight, up_scale, down_weight, down_scale):
    def line(a):
        return a.reshape(1, -1)

    hbm = pl.BlockSpec(memory_space=pl.ANY)
    vmem = pl.BlockSpec(memory_space=pltpu.VMEM)
    V = pltpu.VMEM
    return pl.pallas_call(
        functools.partial(kernel, n_events=N_EVENTS),
        out_shape=V((256, T), F32),
        in_specs=[hbm] * 19,
        out_specs=vmem,
        scratch_shapes=[
            V((4, 8, 64, NM), BF), V((4, 8, 64, G1L), BF), V((4, 8, 64, G2L), BF),
            V((4, 8, 64, D1L), BF), V((4, 8, 64, D2L), BF),
            V((8, T, 256), BF), V((8, T, 256), BF), V((T, 2048), BF), V((T, D1L + D2L), BF),
            V((8, T), F32), V((T, 128), BF), V((4, 256, T), F32),
            V((4, ST, T), BF), V((4, ST, T), BF), V((3, ST, T), BF), V((3, ST, T), BF),
            V((4, 4, 64, T), BF), V((4, 4, 64, T), BF), V((4, 3, 64, T), BF), V((4, 3, 64, T), BF),
            V((256, T), BF), V((1, 2048), F32), V((1, 2048), F32), V((64, 64), F32), V((64, 64), F32),
            V((64, 64), F32), V((64, 64), F32), V((64, FFL), F32), V((64, FFL), F32), V((64, FFL), F32),
            V((1, 64), F32), V((1, 64), F32), V((1, 64), F32), V((3, 64), F32), V((1, 64), F32), V((1, 64), F32),
            V((FFL,), F32), V((FFL,), F32), V((1, 64), F32), V((8, 128), F32),
            pltpu.SemaphoreType.DMA((N_OUT,)), pltpu.SemaphoreType.DMA((N_IN,)),
            pltpu.SemaphoreType.DMA((19,)),
        ],
        compiler_params=pltpu.CompilerParams(collective_id=0, has_side_effects=True,
                                             vmem_limit_bytes=60 * 1024 * 1024),
        name="layer",
    )(residual, line(mixer_gain), line(channel_gain), value_weight, input_gate_weight, output_gate_weight,
      mixer_out_weight, gate_weight, up_weight, down_weight.T, line(value_scale), line(input_gate_scale),
      line(output_gate_scale), conv_taps, line(conv_gain), line(mixer_out_scale), gate_scale,
      up_scale, line(down_scale)).astype(BF)


def solution(mesh):
    rf = ("rep", "fs")
    in_specs = (P("tp", rf), P(), P("fs", "tp"), P("tp"), P("fs", "tp"), P("tp"), P("fs", "tp"), P("tp"),
                P(None, "tp"), P("tp"), P("tp", "fs"), P("fs"), P(), P("fs", "tp"), P("tp"), P("fs", "tp"),
                P("tp"), P("tp", "fs"), P("fs"))
    return jax.shard_map(local, mesh=mesh, in_specs=in_specs, out_specs=P("tp", rf), check_vma=False)
```

```python
import functools

import jax
import jax.numpy as jnp
from jax import lax
from jax.experimental import pallas as pl
from jax.experimental.pallas import tpu as pltpu
from jax.sharding import PartitionSpec as P

MESH = pl.DeviceIdType.MESH
F32 = jnp.float32
BF = jnp.bfloat16
EPS = 1e-06
LEN = 128
T = 256
NM, G1L, G2L, D1L, D2L = 256, 1024, 384, 256, 384
FFL = 704
DROWS = 80
ST = 272


class Event:
    def __init__(self, name, link, size, deps, put, got):
        self.name, self.link, self.size, self.deps = name, link, size, deps
        self.put, self.got = put, got


RATE = {"p": 90.0, "xx": 25.0, "x+": 40.0}
LAT = {"p": 1.7, "xx": 2.8}


def landing(name):
    kind, last = name[0], name[-1]
    if kind == "G" and "z" in name and last == "2":
        return "Gz2"
    if kind == "E" and "z" in name and last == "2":
        return f"Ez2{int(name[1:name.index('z')]) % 4}"
    if kind in "MHDmhd" and "y" in name and last == "4":
        return kind.upper() + "y4"
    if kind == "X" and name[2] == "p":
        return name[:3]
    if kind in "RU":
        return name[:1 if kind == "R" else 2]
    return name


def leaving(name):
    if name[0] in "XQRSU":
        return name[:2] if name[0] == "X" else name[0]
    return name[0].upper() + ("z" if "z" in name else "y")


def plan(events, tasks):
    done, order, sent, flights = set(), [], set(), []
    passed_on = {d for e in events for d in e.deps}
    by_name = {e.name: e for e in events}
    waited = set()
    free = {}
    now = 0.0

    def launch():
        for e in events:
            if e.name not in sent and all(d in done for d in e.deps):
                sent.add(e.name)
                start = max(now, free.get(e.link[:2], 0.0))
                end = start + e.size / (RATE.get(e.link, 46.0) * 1e3)
                free[e.link[:2]] = end
                flights.append((end + LAT.get(e.link, 2.0), e))
                order.append(("send", e))

    launch()
    left = list(tasks)
    while flights or left:
        ready = [t for t in left if all(d in done for d in t[1])]
        landed = [f for f in flights if f[0] <= now]
        if landed:
            f = min(landed, key=lambda v: v[0])
        elif ready:
            t = ready[0]
            left.remove(t)
            for d in t[1]:
                if d in by_name and landing(d) not in waited:
                    waited.add(landing(d))
                    order.append(("wait", by_name[d]))
            order.append(("run", t))
            now += t[2]
            done.add(t[0])
            launch()
            continue
        else:
            f = min(flights, key=lambda v: v[0])
            now = f[0]
        flights.remove(f)
        if f[1].name in passed_on and landing(f[1].name) not in waited:
            waited.add(landing(f[1].name))
            order.append(("wait", f[1]))
        done.add(f[1].name)
        launch()
    return order


def weight_events(M, G1, G2, D1, D2, W):
    ev = []

    def add(name, link, size, deps, ref):
        ev.append(Event(name, link, size, deps, lambda: ref(*W.shift[link]), lambda: ref(0, 0)))

    def along_z(tag, buf, width, b, have):
        rows = buf.shape[2]
        mid = 32 if rows == 64 else 48
        have = have or CAST.get(tag[0], [])
        size = rows * width * 2
        for sign, link in ((-1, "z+"), (1, "z-")):
            add(f"{tag}{link}1", link, size, have, lambda dz, dy, s=sign: buf.at[W.zl(s + dz), W.yy(b + dy)])
        for sign, link, lo, n in ((-1, "z+", 0, mid), (1, "z-", mid, rows - mid)):
            if tag == "M":
                ev.append(Event(f"{tag}{link}2", link + link[1], 2 * n * width * 2, [],
                                lambda lo=lo, n=n: buf.at[W.zl(0), W.yy(0), pl.ds(lo, n)],
                                lambda s=sign, lo=lo, n=n: buf.at[W.zl(2 * s), W.yy(0), pl.ds(lo, n)]))
                continue
            add(f"{tag}{link}2", link, n * width * 2, [f"{tag}{link}1"],
                lambda dz, dy, s=sign, lo=lo, n=n: buf.at[W.zl(2 * s + dz), W.yy(b + dy), pl.ds(lo, n)])
        return [f"{tag}z+1", f"{tag}z-1", f"{tag}z+2", f"{tag}z-2"]

    def gate(tag, s, link):
        other = GATE.get(f"{tag}{s}")
        if not other:
            return []
        kind = other[0]
        if other[1] == "4" and kind in "MHD" and link == "y-":
            kind = kind.lower()
        return [f"{kind}{link}{other[1]}"]

    def columns_along_y(tag, buf, width, first):
        names = []
        for s in (1, 2, 3, 4):
            for t, at in ((tag, 0), (tag.lower(), 2)):
                for sign, link in ((-1, "y+"), (1, "y-")):
                    if s == 4 and (t == tag) != (link == "y+"):
                        continue
                    add(f"{t}{link}{s}", link, 2 * buf.shape[2] * width * 2,
                        (first if s == 1 else [f"{t}{link}{s - 1}"]) + gate(tag, s, link),
                        lambda dz, dy, s=s, sign=sign, at=at: buf.at[pl.ds(at, 2), W.yy(sign * s + dy)])
                    names.append(f"{t}{link}{s}")
        return names

    def own_along_y(tag, buf, width):
        for s in (1, 2, 3, 4):
            for sign, link, lo in ((-1, "y+", 0), (1, "y-", 32)):
                n, at = (64, 0) if s < 4 else (32, lo)
                add(f"{tag}{link}{s}", link, n * width * 2,
                    (CAST[tag] if s == 1 else [f"{tag}{link}{s - 1}"]) + gate(tag, s, link),
                    lambda dz, dy, s=s, sign=sign, at=at, n=n: buf.at[W.zl(dz), W.yy(sign * s + dy), pl.ds(at, n)])

    def behind(tag, b):
        if b == 0:
            return []
        if b == 4:
            return [f"{tag}y+4", f"{tag}y-4"]
        return [f"{tag}y+{-b}"] if b < 0 else [f"{tag}y-{b}"]

    def z_names(tag):
        return [f"{tag}z+1", f"{tag}z-1", f"{tag}z+2", f"{tag}z-2"]

    need = {}
    of_y = {0: z_names("D"), 4: ["Dy+4", "dy-4"]}
    for s in (1, 2, 3):
        of_y[-s] = [f"Dy+{s}", f"dy+{s}"]
        of_y[s] = [f"Dy-{s}", f"dy-{s}"]
    for part in FIRST:
        if part == "M":
            need["M"] = along_z("M", M, NM, 0, []) + columns_along_y("M", M, NM, z_names("M"))
        elif part == "G":
            own_along_y("G", G1, G1L)
        elif part == "E":
            own_along_y("E", D2, D2L)
        elif part == "Hz":
            along_z("H", G2, G2L, 0, [])
        elif part == "Dz":
            along_z("D", D1, D1L, 0, [])
        elif part == "H":
            need["H"] = z_names("H") + columns_along_y("H", G2, G2L, z_names("H"))
        elif part == "D":
            columns_along_y("D", D1, D1L, z_names("D"))
        elif part == "Gz":
            need["G"] = []
            for b in (0, -1, 1, -2, 2, -3, 3, 4):
                need["G"] += behind("G", b) + along_z(f"G{b}", G1, G1L, b, behind("G", b))
        else:
            for b in LAST:
                of_y[b] = of_y[b] + behind("E", b) + along_z(f"E{b}", D2, D2L, b, CAST["E"] + behind("E", b) + z_names(HOLD)[:2])
    return ev, need["M"], need["G"], need["H"], of_y


CAST = {"G": ["castG"], "H": ["castG"], "D": ["castD"], "E": ["castD"]}
FIRST = ("Ez", "D", "Hz", "M", "Gz", "E", "H", "G", "Dz")
LAST = (0, -2, 2, 4, -3, 3, -1, 1)
HOLD = "G4"
GROUPS = (2, 1, 0, 3)
GATE = {
    "H1": "G4", "D2": "H3", "E1": "G3", "D3": "D2", "D1": "E2", "H3": "H2", "E2": "M2", "G4": "G2", "E3":
    "H1", "H2": "M4", "M2": "M1",
}


class Where:
    pass


def kernel(res_in, mgain_in, cgain_in, v_in, i_in, o_in, w_in, g_in, u_in, d_in,
           vs_in, is_in, os_in, taps_in, cg_in, ms_in, gs_in, us_in, ds_in, out,
           M, G1, G2, D1, D2, X1, X2, XN, hid, keep, mixed_to, own32, preo, prei, rxo, rxi, qo, qi, ro, ri,
           res, mgain, cgain, vw, iw, ow, mw, gw, uw, dw, vs, ivs, ovs, taps, cg, ms, gs, us, ds, small,
           send_sem, recv_sem, loc_sem, n_events):
    rep, fs, tp = lax.axis_index("rep"), lax.axis_index("fs"), lax.axis_index("tp")
    y, zl = lax.rem(fs, 8), lax.div(fs, 8)
    x, c = lax.div(tp, 2), lax.rem(tp, 2)
    z = rep * 4 + zl

    def y_at(d):
        return {"fs": zl * 8 + lax.rem(y + d + 8, 8)}

    def z_at(d):
        zz = lax.rem(z + d + 8, 8)
        return {"rep": lax.div(zz, 4), "fs": lax.rem(zz, 4) * 8 + y}

    def x_at(d):
        return {"tp": lax.rem(x + d + 4, 4) * 2 + c}

    partner = {"tp": x * 2 + 1 - c}
    target = {"y+": y_at(1), "y-": y_at(-1), "z+": z_at(1), "z-": z_at(-1), "z++": z_at(2), "z--": z_at(-2),
              "x+": x_at(1), "x-": x_at(-1), "xx": x_at(2), "p": partner}

    W = Where()
    W.shift = {"y+": (0, 1), "y-": (0, -1), "z+": (1, 0), "z-": (-1, 0)}
    W.zl = lambda d: lax.rem(zl + d + 8, 4)
    W.yy = lambda d: lax.rem(y + d + 16, 8)

    ev, all_m, all_g, all_h, of_y = weight_events(M, G1, G2, D1, D2, W)
    pos = {"x+": -1, "x-": 1, "xx": 2}

    def slot(d, core):
        return lax.rem(x + d + 4, 4) * 2 + core

    def spread(tag, buf, first):
        names = []
        for link in ("x+", "x-", "xx"):
            ev.append(Event(f"{tag}{link}", link, T * 256 * 2, [first] if first else [],
                            lambda: buf.at[slot(0, c)], lambda link=link: buf.at[slot(pos[link], c)]))
            names.append(f"{tag}{link}")
        ev.append(Event(f"{tag}p", "p", T * 256 * 2, [first] if first else [],
                        lambda: buf.at[slot(0, c)], lambda: buf.at[slot(0, 1 - c)]))
        names.append(f"{tag}p")
        for link in ("x+", "x-", "xx"):
            ev.append(Event(f"{tag}p{link}", "p", T * 256 * 2, [f"{tag}{link}"],
                            lambda link=link: buf.at[slot(pos[link], c)],
                            lambda link=link: buf.at[slot(pos[link], 1 - c)]))
            names.append(f"{tag}p{link}")
        return names

    all_x1 = spread("X1", X1, None)
    hop = {"x+": 1, "x-": 3, "xx": 2}
    for j in (2, 1, 3, 0):
        ev.append(Event(f"Q{j}", "p", ST * T * 2, [f"mix{j}"], lambda j=j: preo.at[j], lambda j=j: prei.at[j]))
    for link, j in (("xx", 2), ("x+", 1), ("x-", 3)):
        ev.append(Event(f"R{link}", link, ST * T * 2, [f"mixsum{j}"],
                        lambda j=j: rxo.at[j - 1], lambda j=j: rxi.at[j - 1]))
    all_x2 = spread("X2", X2, "after")
    for g in range(4):
        ev.append(Event(f"S{g}", "p", 256 * T * 2, [f"down{g}"], lambda g=g: qo.at[g], lambda g=g: qi.at[g]))
        for link, j in hop.items():
            ev.append(Event(f"U{g}{link}", link, 64 * T * 2, [f"sum{g}"],
                            lambda j=j, g=g: ro.at[g, j - 1], lambda j=j, g=g: ri.at[g, j - 1]))
    assert len(ev) == n_events, len(ev)

    barrier = pltpu.get_barrier_semaphore()
    for dev in target.values():
        pl.semaphore_signal(barrier, inc=1, device_id=dev, device_id_type=MESH)

    ins = [(res_in, res), (v_in, vw), (i_in, iw), (o_in, ow), (w_in, mw), (ms_in, ms), (g_in, gw), (u_in, uw),
           (d_in, dw), (ds_in, ds), (mgain_in, mgain), (cgain_in, cgain), (vs_in, vs), (is_in, ivs), (os_in, ovs),
           (taps_in, taps), (cg_in, cg), (gs_in, gs), (us_in, us)]
    copies = [pltpu.make_async_copy(src, dst, loc_sem.at[i]) for i, (src, dst) in enumerate(ins)]
    for copy in copies:
        copy.start()
    def ready(*which):
        for i in which:
            copies[i].wait()

    own = (zl, y)
    ready(0, 1, 2, 3, 4, 5)
    X1[slot(0, c)] = res[...].astype(F32).T.astype(BF)
    M[(*own, slice(None), slice(0, 128))] = jnp.concatenate([vw[...], iw[...]], axis=1).astype(BF)
    turned = (mw[...] * ms[...]).T
    M[(*own, slice(None), slice(128, 256))] = jnp.concatenate([ow[...], turned], axis=1).astype(BF)

    def cast_gate_up():
        ready(6, 7)
        half = lax.broadcasted_iota(jnp.int32, (64, 128), 1) < 64
        for t in range(6):
            if t < 5:
                gate, up = gw[:, 128 * t:128 * t + 128], uw[:, 128 * t:128 * t + 128]
            else:
                gate = jnp.concatenate([gw[:, 640:704]] * 2, axis=1)
                up = jnp.concatenate([uw[:, 640:704]] * 2, axis=1)
            turn = pltpu.roll(up, 64, axis=1)
            pair = [jnp.where(half, gate, turn).astype(BF), jnp.where(half, turn, gate).astype(BF)]
            for k in range(2 if t < 5 else 1):
                n = 2 * t + k
                if n < G1L // 128:
                    G1[(*own, slice(None), slice(128 * n, 128 * n + 128))] = pair[k]
                else:
                    n -= G1L // 128
                    G2[(*own, slice(None), slice(128 * n, 128 * n + 128))] = pair[k]

    def cast_down():
        ready(8, 9)
        rescale = ds[...].T
        D1[(*own, slice(0, 64))] = (dw[:, 0:256] * rescale).astype(BF)
        D2[own] = (dw[:, 256:640] * rescale).astype(BF)
        tail = dw[:, 640:704] * rescale
        fold = [jnp.concatenate([tail[32 * k:32 * k + 16], tail[32 * k + 16:32 * k + 32]], axis=1) for k in range(2)]
        D1[(*own, slice(64, 80))] = jnp.concatenate(fold, axis=1).astype(BF)
        ready(*range(10, 19))
        row = vs[...] * ivs[...] * ovs[...]
        for k in range(3):
            line = taps[k:k + 1] * row
            small[k:k + 1] = jnp.concatenate([line, line], axis=1)
        small[3:4] = jnp.concatenate([cg[...], cg[...]], axis=1)

    pl.semaphore_wait(barrier, 10)

    bufs = {"M": M, "G": G1, "H": G2, "D": D1, "E": D2}
    out_total = {"X1": X1.at[:7], "X2": X2.at[:7], "Q": preo, "R": rxo, "S": qo, "U": ro}
    in_total = {"Gz2": G1.at[0], "X1p": X1.at[:4], "X2p": X2.at[:4], "R": rxi}
    for k, buf in bufs.items():
        if k in "MHD":
            out_total[k + "z"], out_total[k + "y"] = buf.at[0, :3], buf.at[:, :7]
            in_total[k + "y4"] = buf.at[:, 0]
        else:
            out_total[k + "z"], out_total[k + "y"] = buf.at[:3], buf.at[0, :7]
    for g in range(4):
        in_total[f"Ez2{g}"] = D2.at[0, :2]
        in_total[f"U{g}"] = ri.at[g]
    out_index = {k: i for i, k in enumerate(out_total)}
    in_index = {k: i for i, k in enumerate(dict.fromkeys(landing(e.name) for e in ev))}
    assert len(out_index) == N_OUT and len(in_index) == N_IN, (len(out_index), len(in_index))

    def start(e):
        ref = e.put()
        pltpu.make_async_remote_copy(
            src_ref=ref, dst_ref=ref if e.link[0] in "yz" or e.name[:1] == "X" else e.got(),
            send_sem=send_sem.at[out_index[leaving(e.name)]], recv_sem=recv_sem.at[in_index[landing(e.name)]],
            device_id=target[e.link], device_id_type=MESH).start()

    def arrive(e):
        key = landing(e.name)
        ref = in_total[key] if key in in_total else e.got()
        pltpu.make_async_remote_copy(src_ref=ref, dst_ref=ref, send_sem=send_sem.at[0],
                                     recv_sem=recv_sem.at[in_index[key]],
                                     device_id=target[e.link], device_id_type=MESH).wait_recv()

    def left():
        for key, i in out_index.items():
            ref = out_total[key]
            pltpu.make_async_remote_copy(src_ref=ref, dst_ref=ref, send_sem=send_sem.at[i], recv_sem=recv_sem.at[0],
                                         device_id=partner, device_id_type=MESH).wait_send()

    def normed(buf, gain):
        def square(k, s):
            v = buf[k].astype(F32)
            return s + v * v
        total = lax.fori_loop(0, 8, square, jnp.zeros((T, 256), F32))
        factor = lax.rsqrt(jnp.sum(total, axis=1, keepdims=True) * (1.0 / 2048) + EPS)
        for k in range(8):
            cols = slice(k * 256, k * 256 + 256)
            XN[:, cols] = (buf[k].astype(F32) * factor * gain[0:1, cols]).astype(BF)

    def norm_one():
        normed(X1, mgain)

    def split_stats(s):
        high = s.astype(BF)
        low = (s - high.astype(F32)).astype(BF)
        return jnp.concatenate([high, low], axis=0)

    def mix():
        proj = jnp.dot(XN[...], M[...].reshape(2048, NM), preferred_element_type=F32)
        first, second = proj[:, :128], proj[:, 128:]
        u = first * pltpu.roll(first, 64, axis=1)
        place = lax.rem(lax.broadcasted_iota(jnp.int32, (T, 128), 0), LEN)
        lane = lax.broadcasted_iota(jnp.int32, (T, 128), 1)
        one = jnp.where(place >= 1, pltpu.roll(u, 1, axis=0), 0.0)
        two = jnp.where(place >= 2, pltpu.roll(u, 2, axis=0), 0.0)
        conv = small[2:3] * u + small[1:2] * one + small[0:1] * two
        mixed = jnp.where(lane >= 64, pltpu.roll(second, 64, axis=1) * conv, 0.0)
        sq = mixed * mixed
        high = sq.astype(BF)
        low = (sq - high.astype(F32)).astype(BF)
        ones = jnp.ones((16, 128), BF)
        nt = (((1,), (1,)), ((), ()))
        stat = (lax.dot_general(ones, high, nt, preferred_element_type=F32)
                + lax.dot_general(ones, low, nt, preferred_element_type=F32))[:8]
        scaled = (mixed * small[3:4]).T.astype(BF)
        mixed_to[...] = scaled
        keep[0:8] = stat

    def mix_for(j):
        for mine in (False, True):
            core = c if mine else 1 - c
            w = M[lax.rem(x + j, 4), pl.ds(4 * core, 4), :, 128:].reshape(256, 128)
            part = jnp.dot(w, mixed_to[...], preferred_element_type=F32)
            if mine:
                own32[j] = part
            else:
                preo[j, :256] = part.astype(BF)
                preo[j, 256:] = split_stats(keep[0:8])

    def mix_first():
        mix()
        mix_for(2)

    def mixsum(j):
        stat = keep[0:8] + prei[j, 256:264].astype(F32) + prei[j, 264:272].astype(F32)
        rxo[j - 1, :256] = (own32[j] + prei[j, :256].astype(F32)).astype(BF)
        rxo[j - 1, 256:] = split_stats(stat)

    def after():
        stat = keep[0:8] + prei[0, 256:264].astype(F32) + prei[0, 264:272].astype(F32)
        total = own32[0] + prei[0, :256].astype(F32)
        for j in range(3):
            total = total + rxi[j, :256].astype(F32)
            stat = stat + rxi[j, 256:264].astype(F32) + rxi[j, 264:272].astype(F32)
        factor = lax.rsqrt(stat * (1.0 / 512) + EPS)[0:1]
        value = (res[...].astype(F32) + total * factor).astype(BF)
        X2[slot(0, c)] = value.astype(F32).T.astype(BF)
        out[...] = value.astype(F32)

    def norm_two():
        normed(X2, cgain)

    lane = lax.broadcasted_iota(jnp.int32, (T, 128), 1)

    def hidden_tiles(w, first, tiles):
        z = jnp.dot(XN[...], w, preferred_element_type=F32)
        for k in range(0, tiles, 2):
            n = (first + k) // 2
            even = z[:, 128 * k:128 * k + 128]
            if k + 1 < tiles:
                odd = z[:, 128 * k + 128:128 * k + 256]
                gsc, usc = (v[128 * n:128 * n + 128].reshape(1, 128) for v in (gs, us))
            else:
                odd = jnp.zeros((T, 128), F32)
                gsc = jnp.concatenate([gs[640:704].reshape(1, 64)] * 2, axis=1)
                usc = jnp.concatenate([us[640:704].reshape(1, 64)] * 2, axis=1)
            gate = jnp.where(lane < 64, even, odd) * gsc
            up = pltpu.roll(jnp.where(lane < 64, odd, even), 64, axis=1) * usc
            value = gate / (1.0 + jnp.exp(-gate)) * up
            hid[128 * n:128 * n + 128] = value.T.astype(BF)

    def hidden_one():
        for n in range(4):
            hidden_tiles(G1[:, :, :, n * 256:n * 256 + 256].reshape(2048, 256), 2 * n, 2)

    def hidden_two():
        hidden_tiles(G2[:, :, :, 0:256].reshape(2048, 256), 8, 2)
        hidden_tiles(G2[:, :, :, 256:384].reshape(2048, 128), 10, 1)

    def down(g, core):
        at = lax.rem(y + g, 4) + 4 * core
        p = jnp.dot(D1[:, at, :64].reshape(256, D1L), hid[:D1L], preferred_element_type=F32)
        q = jnp.dot(D2[:, at].reshape(256, D2L), hid[D1L:D1L + D2L], preferred_element_type=F32)
        fold = [D1[:, at, 64:, 128 * k:128 * k + 128].astype(F32) for k in range(2)]
        flat = []
        for f in fold:
            flat += [f, pltpu.roll(f.reshape(64, 128), 64, axis=1).reshape(4, 16, 128)]
        tail = jnp.concatenate(flat, axis=1).reshape(256, 128).astype(BF)
        r = jnp.dot(tail, hid[D1L + D2L:], preferred_element_type=F32)
        return (p + q + r).reshape(4, 64, T)

    def down_partner(g):
        qo[g] = down(g, 1 - c).astype(BF)

    def down_own(g):
        own32[g] = down(g, c).reshape(256, T)

    def sum_for(g):
        for j in (2, 1, 3):
            x_to = lax.rem(x + j, 4)
            ro[g, j - 1] = (own32[g, pl.ds(pl.multiple_of(x_to * 64, 64), 64)] + qi[g, x_to].astype(F32)).astype(BF)

    def final(g):
        rows = pl.ds(pl.multiple_of(lax.rem(y + g, 4) * 64, 64), 64)
        total = own32[g, pl.ds(pl.multiple_of(x * 64, 64), 64)] + qi[g, x].astype(F32)
        for j in range(3):
            total = total + ri[g, j].astype(F32)
        out[rows] = out[rows] + total

    tasks = [
        ("castG", [], 0.4, cast_gate_up),
        ("castD", ["castG"], 0.4, cast_down),
        ("norm1", all_x1, 0.8, norm_one),
        ("mix2", ["norm1"] + all_m, 1.0, mix_first),
        ("mix1", ["mix2"], 0.2, lambda: mix_for(1)),
        ("mix3", ["mix1"], 0.2, lambda: mix_for(3)),
        ("mix0", ["mix3"], 0.2, lambda: mix_for(0)),
        ("mixsum2", ["Q2", "mix0"], 0.05, lambda: mixsum(2)),
        ("mixsum1", ["Q1", "mix0"], 0.05, lambda: mixsum(1)),
        ("mixsum3", ["Q3", "mix0"], 0.05, lambda: mixsum(3)),
        ("after", ["Q0", "mixsum2", "mixsum1", "mixsum3", "Rx+", "Rx-", "Rxx"], 0.2, after),
        ("norm2", all_x2, 0.8, norm_two),
        ("hidden1", ["norm2"] + all_g, 1.4, hidden_one),
        ("hidden2", ["norm2"] + all_h, 0.8, hidden_two),
    ]
    for g in GROUPS:
        need = of_y[g] + (of_y[g - 4] if g else of_y[4])
        tasks.append((f"down{g}", ["hidden1", "hidden2"] + need, 0.4, lambda g=g: down_partner(g)))
        tasks.append((f"own{g}", [f"down{g}"], 0.4, lambda g=g: down_own(g)))
        tasks.append((f"sum{g}", [f"own{g}", f"S{g}"], 0.2, lambda g=g: sum_for(g)))
    for g in GROUPS:
        tasks.append((f"final{g}", [f"U{g}x+", f"U{g}x-", f"U{g}xx"], 0.1, lambda g=g: final(g)))
    order = plan(ev, tasks)
    for kind, item in order:
        if kind == "send":
            start(item)
        elif kind == "wait":
            arrive(item)
        else:
            item[3]()
    left()


N_EVENTS = 18 + 40 + 18 + 18 + 40 + 7 + 4 + 3 + 7 + 4 + 12
N_OUT, N_IN = 16, 125


def local(residual, mixer_gain, value_weight, value_scale, input_gate_weight, input_gate_scale,
          output_gate_weight, output_gate_scale, conv_taps, conv_gain, mixer_out_weight, mixer_out_scale,
          channel_gain, gate_weight, gate_scale, up_weight, up_scale, down_weight, down_scale):
    def line(a):
        return a.reshape(1, -1)

    hbm = pl.BlockSpec(memory_space=pl.ANY)
    vmem = pl.BlockSpec(memory_space=pltpu.VMEM)
    V = pltpu.VMEM
    return pl.pallas_call(
        functools.partial(kernel, n_events=N_EVENTS),
        out_shape=V((256, T), F32),
        in_specs=[hbm] * 19,
        out_specs=vmem,
        scratch_shapes=[
            V((4, 8, 64, NM), BF), V((4, 8, 64, G1L), BF), V((4, 8, 64, G2L), BF),
            V((4, 8, DROWS, D1L), BF), V((4, 8, 64, D2L), BF),
            V((8, T, 256), BF), V((8, T, 256), BF), V((T, 2048), BF), V((D1L + D2L + 128, T), BF),
            V((8, T), F32), V((128, T), BF), V((4, 256, T), F32),
            V((4, ST, T), BF), V((4, ST, T), BF), V((3, ST, T), BF), V((3, ST, T), BF),
            V((4, 4, 64, T), BF), V((4, 4, 64, T), BF), V((4, 3, 64, T), BF), V((4, 3, 64, T), BF),
            V((256, T), BF), V((1, 2048), F32), V((1, 2048), F32), V((64, 64), F32), V((64, 64), F32),
            V((64, 64), F32), V((64, 64), F32), V((64, FFL), F32), V((64, FFL), F32), V((64, FFL), F32),
            V((1, 64), F32), V((1, 64), F32), V((1, 64), F32), V((3, 64), F32), V((1, 64), F32), V((1, 64), F32),
            V((FFL,), F32), V((FFL,), F32), V((1, 64), F32), V((8, 128), F32),
            pltpu.SemaphoreType.DMA((N_OUT,)), pltpu.SemaphoreType.DMA((N_IN,)),
            pltpu.SemaphoreType.DMA((19,)),
        ],
        compiler_params=pltpu.CompilerParams(collective_id=0, has_side_effects=True,
                                             vmem_limit_bytes=60 * 1024 * 1024),
        name="layer",
    )(residual, line(mixer_gain), line(channel_gain), value_weight, input_gate_weight, output_gate_weight,
      mixer_out_weight, gate_weight, up_weight, down_weight.T, line(value_scale), line(input_gate_scale),
      line(output_gate_scale), conv_taps, line(conv_gain), line(mixer_out_scale), gate_scale,
      up_scale, line(down_scale)).astype(BF)


def solution(mesh):
    rf = ("rep", "fs")
    in_specs = (P("tp", rf), P(), P("fs", "tp"), P("tp"), P("fs", "tp"), P("tp"), P("fs", "tp"), P("tp"),
                P(None, "tp"), P("tp"), P("tp", "fs"), P("fs"), P(), P("fs", "tp"), P("tp"), P("fs", "tp"),
                P("tp"), P("tp", "fs"), P("fs"))
    return jax.shard_map(local, mesh=mesh, in_specs=in_specs, out_specs=P("tp", rf), check_vma=False)
```
